128 devices in a mesh: ep: 64 (over z, y, x), tp: 2 (over core).
Axes of the slice: x: 4, y: 4, z: 4, core: 2. Of those that a mesh axis runs over, the one named last changes fastest.
Arguments:
- tokens: bfloat16 [1536, 2048], P('ep'), may hold values from -6 to 6
- norm_gain: bfloat16 [2048], replicated, may hold values from 0.099609375 to 1.8984375
- query_w: bfloat16 [2048, 1024], P(None, 'tp'), may hold values from -0.125 to 0.125
- key_w: bfloat16 [2048, 128], replicated, may hold values from -0.125 to 0.125
- value_w: bfloat16 [2048, 128], replicated, may hold values from -0.125 to 0.125
- forget_w: bfloat16 [2048, 16], replicated, may hold values from -0.125 to 0.125
- forget_bias: float32 [16], replicated, may hold values from 0 to 4
- query_gain: bfloat16 [64], replicated, may hold values from 0.099609375 to 1.8984375
- key_gain: bfloat16 [64], replicated, may hold values from 0.099609375 to 1.8984375
- cache_key: bfloat16 [1536, 2, 64, 1024], P('ep', 'tp'), may hold values from -6 to 6
- cache_value: bfloat16 [1536, 2, 64, 1024], P('ep', 'tp'), may hold values from -6 to 6
- cache_gate: float32 [1536, 16, 1024], P('ep', 'tp'), may hold values from -105 to 0, as said below
- cache_len: int32 [1536], P('ep'), may hold values from 256 to 1024
- out_w: bfloat16 [1024, 2048], P('tp'), may hold values from -0.1875 to 0.1875
- post_gain: bfloat16 [2048], replicated, may hold values from 0.099609375 to 1.8984375
- branch_gate: bfloat16 [2048], replicated, may hold values from -0.125 to 0.125
- dense_gate_w: bfloat16 [2048, 16384], P(None, ('ep', 'tp')), may hold values from -0.125 to 0.125
- dense_up_w: bfloat16 [2048, 16384], P(None, ('ep', 'tp')), may hold values from -1.3258252 to 1.3258252
- dense_down_w: bfloat16 [16384, 2048], P(('ep', 'tp')), may hold values from -0.046875 to 0.046875
- expert_choice: int32 [1536, 2], P('ep'), may hold values from 0 to 63, as said below
- route_weight: float32 [1536, 2], P('ep'), may hold values from 0.1 to 1
- expert_gate_w: bfloat16 [64, 2048, 1024], P('ep', None, 'tp'), may hold values from -0.125 to 0.125
- expert_up_w: bfloat16 [64, 2048, 1024], P('ep', None, 'tp'), may hold values from -0.125 to 0.125
- expert_down_w: bfloat16 [64, 1024, 2048], P('ep', 'tp'), may hold values from -0.1875 to 0.1875
Outputs:
- mixed_out: bfloat16 [1536, 2048], P('ep', 'tp')
- fresh_key: bfloat16 [1536, 2, 64], P('ep', 'tp')
- fresh_value: bfloat16 [1536, 2, 64], P('ep', 'tp')
- fresh_gate: float32 [1536, 16], P('ep', 'tp')
The draws below stay inside these ranges and needn't reach their ends.
Inputs may be any that keep to these rules, and one draw needn't show every extreme that they name: `cache_gate`: Non-increasing along positions. `expert_choice`: experts 16 * g to 16 * g + 15 form group g. A token names 2 different experts of one group. Among the 24 tokens of one index of ep, those at even offsets all choose one group and the others choose other groups; no expert is named more than 2 times by them, and some expert exactly 2 times.
All inputs are finite; a program needn't handle non-finite values.
Results may differ from the reference program's by a relative error of at most 0.014.
Values may be sent and summed in bfloat16 or wider, within the bound.
No kernel may reach another device: no remote copies, remote signals or barrier semaphores. Data moves between devices by JAX's collectives and lax.ppermute only.
A program may use at most 128 MiB of HBM per device.

```python
import math
import jax
import jax.numpy as jnp
from jax import lax

D = 2048
HEADS = 16
KV = 2
HD = 64
FFE = 1024
FF2 = 16384
GROUPS = 4
TOPK = 2
SEQ_DEV = 24
STORED_SLOTS = 1024
BATCH_ENTRIES = 1536
EXPERTS = 64
EPG = 16
CAP = 2
N_EP = 64
N_TP = 2


def draw_cache_gate(key, part):
    derived_prng_seeds = jax.random.split(jax.random.fold_in(key, 11), 7)
    fast_share = 0.5
    is_fast = jax.random.uniform(derived_prng_seeds[0], (HEADS,)) < fast_share
    slow_rate = jax.random.uniform(derived_prng_seeds[1], (HEADS,), minval=0.3, maxval=0.8) / STORED_SLOTS
    fast_rate = 1.0 / jax.random.uniform(derived_prng_seeds[2], (HEADS,), minval=30.0, maxval=100.0)
    per_attender_fading = jnp.where(is_fast, fast_rate, slow_rate)
    batch_multiplier = jnp.exp(jax.random.uniform(derived_prng_seeds[3], (BATCH_ENTRIES, 1, 1), minval=math.log(0.6), maxval=math.log(1.6)))
    outer_level_logits = jax.random.uniform(derived_prng_seeds[4], (BATCH_ENTRIES, HEADS, STORED_SLOTS), minval=0.5, maxval=1.5)
    contiguous_first_slot = jax.random.randint(derived_prng_seeds[5], (BATCH_ENTRIES, 3), 0, STORED_SLOTS)
    contiguous_span = jax.random.uniform(derived_prng_seeds[6], (BATCH_ENTRIES, 3), minval=0.22, maxval=0.69)
    current_slot_offset = jnp.arange(STORED_SLOTS)[None, None, :]
    contiguous_tiles = jnp.sum(jnp.where(current_slot_offset == contiguous_first_slot[:, :, None], contiguous_span[:, :, None], 0.0), axis=1)
    increment_fading_exponent = -(per_attender_fading[None, :, None] * batch_multiplier * outer_level_logits) - contiguous_tiles[:, None, :]
    return jnp.cumsum(increment_fading_exponent, axis=2).astype(jnp.float32)


def draw_dense_up_w(key, part):
    base_key = jax.random.fold_in(key, 21)
    column = jnp.arange(FF2, dtype=jnp.float32) / FF2
    entries = jnp.clip(jax.random.normal(base_key, (D, FF2)), -6.0, 6.0)
    column_scale = jnp.exp(math.log(10.0) * column)
    return (entries * column_scale[None, :] * D ** (-0.5)).astype(jnp.bfloat16)


def draw_expert_choice(key, part):
    derived_prng_seeds = jax.random.split(jax.random.fold_in(key, 31), 3)
    blocks = BATCH_ENTRIES // SEQ_DEV
    even_group = jax.random.randint(derived_prng_seeds[0], (blocks, 1), 0, GROUPS)
    other_group = (even_group + 1 + jax.random.randint(derived_prng_seeds[1], (blocks, SEQ_DEV), 0, GROUPS - 1)) % GROUPS
    offset = jnp.arange(SEQ_DEV)[None, :]
    group_id = jnp.where(offset % 2 == 0, even_group, other_group)
    member_of = (group_id[:, :, None] == jnp.arange(GROUPS)[None, None, :]).astype(jnp.int32)
    rank_in = jnp.sum((jnp.cumsum(member_of, axis=1) - member_of) * member_of, axis=2)
    shift_by = jax.random.randint(derived_prng_seeds[2], (blocks, GROUPS), 0, EPG)
    start_at = jnp.sum(member_of * shift_by[:, None, :], axis=2)
    first_member = (start_at + rank_in) % EPG
    second = (first_member + 1) % EPG
    chosen = jnp.stack([group_id * EPG + first_member, group_id * EPG + second], axis=-1)
    return chosen.reshape(BATCH_ENTRIES, TOPK).astype(jnp.int32)


def place_ends(values, stream_key, least, high):
    dims = values.shape
    spot = [jax.random.randint(jax.random.fold_in(stream_key, axis), (), 0, dims[axis]) for axis in range(len(dims))]
    values = values.at[tuple(spot)].set(least)
    longest = dims.index(max(dims))
    spot[longest] = (spot[longest] + 1) % dims[longest]
    return values.at[tuple(spot)].set(high)


def levels(own_key, dims, cuts, smallest, top_value):
    level, own = 1.0, jax.random.fold_in(own_key, 6)
    for axis_at, blocks in cuts:
        steps = jnp.exp(jax.random.uniform(jax.random.fold_in(own, axis_at), (blocks,), jnp.float32, smallest / len(cuts), top_value / len(cuts)))
        level = level * jnp.repeat(steps, dims[axis_at] // blocks).reshape([-1 if axis == axis_at else 1 for axis in range(len(dims))])
    return level


def bell_draw(key, dims, scale, reach, pieces=(), held_as=jnp.bfloat16):
    values = scale * jax.random.normal(key, dims, jnp.float32)
    if pieces:
        values = values * levels(key, dims, pieces, -0.22, 0.18)
    return jnp.clip(values, -reach, reach).astype(held_as)


def setup_inputs(seed: int = 0) -> dict:
    streams_of = jax.random.split(jax.random.key(seed), 25)
    return {
        "tokens": bell_draw(streams_of[0], (BATCH_ENTRIES, D), 1.0, 6.0, ((0, 64),)),
        "norm_gain": jnp.clip(1.0 + 0.18 * jax.random.normal(streams_of[1], (D,), jnp.float32), 0.099609375, 1.8984375).astype(jnp.bfloat16),
        "query_w": bell_draw(streams_of[2], (D, HEADS * HD), D ** -0.5, 0.125, ((1, 2),)),
        "key_w": bell_draw(streams_of[3], (D, KV * HD), D ** -0.5, 0.125),
        "value_w": bell_draw(streams_of[4], (D, KV * HD), D ** -0.5, 0.125),
        "forget_w": bell_draw(streams_of[5], (D, HEADS), D ** -0.5, 0.125),
        "forget_bias": jnp.clip(jax.random.uniform(streams_of[6], (HEADS,), jnp.float32, 0.0, 4.0), 0.0, 4.0),
        "query_gain": jnp.clip(1.0 + 0.18 * jax.random.normal(streams_of[7], (HD,), jnp.float32), 0.099609375, 1.8984375).astype(jnp.bfloat16),
        "key_gain": jnp.clip(1.0 + 0.18 * jax.random.normal(streams_of[8], (HD,), jnp.float32), 0.099609375, 1.8984375).astype(jnp.bfloat16),
        "cache_key": bell_draw(streams_of[9], (BATCH_ENTRIES, KV, HD, STORED_SLOTS), 1.0, 6.0, ((0, 64), (1, 2))),
        "cache_value": bell_draw(streams_of[10], (BATCH_ENTRIES, KV, HD, STORED_SLOTS), 1.0, 6.0, ((0, 64), (1, 2))),
        "cache_gate": draw_cache_gate(jax.random.fold_in(streams_of[24], 71), 0),
        "cache_len": place_ends(jax.random.randint(streams_of[12], (BATCH_ENTRIES,), STORED_SLOTS // 4, STORED_SLOTS + 1), jax.random.fold_in(streams_of[12], 1), STORED_SLOTS // 4, STORED_SLOTS).astype(jnp.int32),
        "out_w": bell_draw(streams_of[13], (HEADS * HD, D), (HEADS * HD) ** -0.5, 0.1875, ((0, 2),)),
        "post_gain": jnp.clip(1.0 + 0.18 * jax.random.normal(streams_of[14], (D,), jnp.float32), 0.099609375, 1.8984375).astype(jnp.bfloat16),
        "branch_gate": bell_draw(streams_of[15], (D,), D ** -0.5, 0.125),
        "dense_gate_w": bell_draw(streams_of[16], (D, FF2), D ** -0.5, 0.125, ((1, 128),)),
        "dense_up_w": draw_dense_up_w(jax.random.fold_in(streams_of[24], 71), 0),
        "dense_down_w": bell_draw(streams_of[18], (FF2, D), FF2 ** -0.5, 0.046875, ((0, 128),)),
        "expert_choice": draw_expert_choice(jax.random.fold_in(streams_of[24], 71), 0),
        "route_weight": jnp.clip(0.1 + 0.9 * jax.random.uniform(streams_of[20], (BATCH_ENTRIES, TOPK), jnp.float32) ** levels(streams_of[20], (BATCH_ENTRIES, TOPK), ((0, 64),), -0.2, 0.2), 0.1, 1.0),
        "expert_gate_w": bell_draw(streams_of[21], (EXPERTS, D, FFE), D ** -0.5, 0.125, ((0, 64), (2, 2))),
        "expert_up_w": bell_draw(streams_of[22], (EXPERTS, D, FFE), D ** -0.5, 0.125, ((0, 64), (2, 2))),
        "expert_down_w": bell_draw(streams_of[23], (EXPERTS, FFE, D), FFE ** -0.5, 0.1875, ((0, 64), (1, 2))),
    }


norm_eps = 1e-06

def rms_scale(values, gain_vec):
    mean_square = lax.optimization_barrier(jnp.mean(values * values, axis=-1, keepdims=True))
    return values * lax.rsqrt(mean_square + norm_eps) * gain_vec

def rounded(values):
    return lax.optimization_barrier(values.astype(jnp.bfloat16)).astype(jnp.float32)

def attend(block_in):
    queries, new_keys, new_values, log_forget, keys_cached, values_cached, gates_cached, lengths = block_in
    row_count = queries.shape[0]
    repeat = HEADS // KV
    score_scale = HD ** (-0.5)
    grouped = queries.reshape(row_count, KV, repeat, HD).astype(jnp.float32)
    scores = jnp.einsum('sgrd,sgdl->sgrl', grouped, keys_cached.astype(jnp.float32)) * score_scale
    own_score = jnp.einsum('sgrd,sgd->sgr', grouped, new_keys.astype(jnp.float32)) * score_scale
    current_slot_offset = lax.broadcasted_iota(jnp.int32, (row_count, STORED_SLOTS), 1)
    at_last = (current_slot_offset == lengths[:, None] - 1)[:, None, :]
    previous = lax.optimization_barrier(jnp.sum(jnp.where(at_last, gates_cached, jnp.zeros_like(gates_cached)), axis=2))
    current = previous + log_forget
    decay_bias = (current[:, :, None] - gates_cached).reshape(row_count, KV, repeat, STORED_SLOTS)
    is_valid = (current_slot_offset < lengths[:, None])[:, None, None, :]
    logits = jnp.where(is_valid, scores + decay_bias, -jnp.inf)
    top_logit = jnp.maximum(lax.optimization_barrier(jnp.max(logits, axis=3)), own_score)
    weights = jnp.exp(logits - top_logit[..., None])
    own_weight = jnp.exp(own_score - top_logit)
    total_weight = lax.optimization_barrier(jnp.sum(weights, axis=3)) + own_weight
    cache_probs = (weights / total_weight[..., None]).astype(jnp.bfloat16)
    own_prob = (own_weight / total_weight).astype(jnp.bfloat16)
    mixed_heads = jnp.einsum('sgrl,sgdl->sgrd', cache_probs.astype(jnp.float32), values_cached.astype(jnp.float32))
    mixed_heads = mixed_heads + own_prob.astype(jnp.float32)[..., None] * new_values.astype(jnp.float32)[:, :, None, :]
    return (mixed_heads.reshape(row_count, HEADS * HD).astype(jnp.bfloat16), current)

def reference(tokens, norm_gain, query_w, key_w, value_w, forget_w, forget_bias, query_gain, key_gain, cache_key, cache_value, cache_gate, cache_len, out_w, post_gain, branch_gate, dense_gate_w, dense_up_w, dense_down_w, expert_choice, route_weight, expert_gate_w, expert_up_w, expert_down_w):
    token_count = tokens.shape[0]
    resid_in = tokens.astype(jnp.float32)
    normed = rms_scale(resid_in, norm_gain.astype(jnp.float32)).astype(jnp.bfloat16)
    queries = jnp.dot(normed, query_w, preferred_element_type=jnp.float32).reshape(token_count, HEADS, HD)
    queries = rms_scale(queries, query_gain.astype(jnp.float32)).astype(jnp.bfloat16)
    fresh_key = jnp.dot(normed, key_w, preferred_element_type=jnp.float32).reshape(token_count, KV, HD)
    fresh_key = rms_scale(fresh_key, key_gain.astype(jnp.float32)).astype(jnp.bfloat16)
    fresh_value = jnp.dot(normed, value_w, preferred_element_type=jnp.float32).astype(jnp.bfloat16).reshape(token_count, KV, HD)
    log_forget = jax.nn.log_sigmoid(jnp.dot(normed, forget_w, preferred_element_type=jnp.float32) + forget_bias)

    def blocks(array_in):
        return array_in.reshape((N_EP, SEQ_DEV) + array_in.shape[1:])
    heads_out, fresh_gate = lax.map(attend, tuple((blocks(array_in) for array_in in (queries, fresh_key, fresh_value, log_forget, cache_key, cache_value, cache_gate, cache_len))))
    heads_out = heads_out.reshape(token_count, HEADS * HD)
    fresh_gate = fresh_gate.reshape(token_count, HEADS)
    head_groups = heads_out.reshape(token_count, N_TP, -1)
    out_parts = out_w.reshape(N_TP, -1, D)
    attn_sum = jnp.zeros((token_count, D), jnp.float32)
    for group_index in range(N_TP):
        attn_sum = attn_sum + rounded(jnp.dot(head_groups[:, group_index], out_parts[group_index], preferred_element_type=jnp.float32))
    resid_out = rounded(resid_in + attn_sum)
    post_norm = rms_scale(resid_out, post_gain.astype(jnp.float32)).astype(jnp.bfloat16)
    branch = jax.nn.sigmoid(jnp.dot(post_norm, branch_gate, preferred_element_type=jnp.float32))
    hidden = jax.nn.silu(jnp.dot(post_norm, dense_gate_w, preferred_element_type=jnp.float32)) * jnp.dot(post_norm, dense_up_w, preferred_element_type=jnp.float32)
    inverse = lax.rsqrt(lax.optimization_barrier(jnp.mean(hidden * hidden, axis=1)) + norm_eps)
    dense_out = rounded(jnp.dot(hidden.astype(jnp.bfloat16), dense_down_w, preferred_element_type=jnp.float32) * inverse[:, None])
    route_total = token_count * TOPK
    route_ids = expert_choice.reshape(-1).astype(jnp.int32)
    limit = N_EP * CAP

    def one_expert(routed_acc, slices):
        gate_mat, up_mat, down_mat, expert_index = slices
        picked = jnp.nonzero(route_ids == expert_index, size=limit, fill_value=route_total)[0].astype(jnp.int32)
        slot_rows = post_norm[jnp.minimum(picked, route_total - 1) // TOPK]
        gate_val = jnp.dot(slot_rows, gate_mat, preferred_element_type=jnp.float32)
        up_val = jnp.dot(slot_rows, up_mat, preferred_element_type=jnp.float32)
        activated = (jax.nn.silu(gate_val) * up_val).astype(jnp.bfloat16)
        act_parts = activated.reshape(limit, N_TP, -1)
        down_parts = down_mat.reshape(N_TP, -1, D)
        expert_out = jnp.zeros((limit, D), jnp.float32)
        for group_index in range(N_TP):
            expert_out = expert_out + rounded(jnp.dot(act_parts[:, group_index], down_parts[group_index], preferred_element_type=jnp.float32))
        routed_acc = routed_acc.at[picked].set(rounded(expert_out), mode='drop')
        return (routed_acc, None)
    routed, _ = lax.scan(one_expert, jnp.zeros((route_total, D), jnp.float32), (expert_gate_w, expert_up_w, expert_down_w, jnp.arange(N_EP, dtype=jnp.int32)))
    expert_sum = lax.optimization_barrier(jnp.sum(route_weight[:, :, None] * routed.reshape(token_count, TOPK, D), axis=1))
    mixed_out = (resid_out + expert_sum + branch[:, None] * dense_out).astype(jnp.bfloat16)
    return (mixed_out, fresh_key, fresh_value, fresh_gate)
```

```python
import functools

import jax
import jax.numpy as jnp
from jax import lax
from jax.experimental import pallas as pl
from jax.experimental.pallas import tpu as pltpu
from jax.sharding import PartitionSpec as P


FF2 = 16384
LANES = 128
INFO = 128
SLOTS = 2
EPS = 1e-06
SWAP = [(0, 1), (1, 0)]
F32 = jnp.float32
BF16 = jnp.bfloat16


def class_of(e):
    return (e ^ (e // 2)) % 2


def swapped(array):
    return lax.ppermute(array, "tp", SWAP)


def iota(shape, dim):
    return lax.broadcasted_iota(jnp.int32, shape, dim)


def mm(a, b):
    return jnp.dot(a, b, preferred_element_type=F32)


def mm_t(a, b):
    return lax.dot_general(a, b, (((1,), (1,)), ((), ())), preferred_element_type=F32)


def silu(v):
    return v / (1.0 + jnp.exp(-v))


def params(limit=56):
    return pltpu.CompilerParams(vmem_limit_bytes=limit << 20)


def whole(shape):
    return pl.BlockSpec(shape, lambda *_: (0,) * len(shape))


def near_call(kernel, arrays, outs, scratch=(), limit=32):
    here = pl.BlockSpec(memory_space=pltpu.VMEM)
    many = isinstance(outs, list)
    return pl.pallas_call(
        kernel,
        in_specs=[here] * len(arrays),
        out_specs=[here] * len(outs) if many else here,
        out_shape=outs,
        scratch_shapes=list(scratch),
        compiler_params=params(limit),
    )(*arrays)


def kept(ref, dim, size, other=False):
    rank = lax.axis_index("tp")
    rank = 1 - rank if other else rank
    at = pl.ds(pl.multiple_of(rank * size, size), size)
    return ref[at, :] if dim == 0 else ref[:, at]


def laid_out(ref):
    rows = ref[...].astype(F32)
    return jnp.concatenate([rows[r : r + 1, :] for r in range(rows.shape[0])], axis=1)


def tiled(vector):
    return vector.reshape(-1, LANES)


def attend_kernel(
    len_ref, tok, ng, qw, kw, vw, fw, fb, qg, kg, key, val, gate, ow,
    partial, fk_out, fv_out, cur_out, q_scr, own_scr, lf_scr, fv_scr, heads_scr, *, block, steps,
):
    step = pl.program_id(0)
    count = tok.shape[0]
    heads = gate.shape[1]
    hd = key.shape[2]
    span = key.shape[3]
    rows = count * heads
    width = heads * hd
    scale = hd ** (-0.5)
    second = lax.axis_index("tp") == 1

    @pl.when(step == 0)
    def _():
        x = tok[...].astype(F32)
        ms = jnp.mean(x * x, axis=1, keepdims=True)
        normed = (x * lax.rsqrt(ms + EPS) * laid_out(ng)).astype(BF16)
        q = mm(normed, qw[...])
        k = mm(normed, kw[...])
        v = mm(normed, vw[...])
        k = jnp.where(second, k[:, hd:], k[:, :hd])
        v = jnp.where(second, v[:, hd:], v[:, :hd]).astype(BF16)
        k = k * lax.rsqrt(jnp.mean(k * k, axis=1, keepdims=True) + EPS) * kg[...].astype(F32)
        k = k.astype(BF16)
        fk_out[...] = k
        fv_out[...] = v
        spread = jnp.broadcast_to(q[:, None, :], (count, heads, width)).reshape(rows, width)
        mine = iota((rows, width), 1) // hd == iota((rows, width), 0) % heads
        spread = jnp.where(mine, spread, 0.0)
        msq = jnp.sum(spread * spread, axis=1, keepdims=True) / hd
        spread = spread * lax.rsqrt(msq + EPS)
        gain = jnp.concatenate([qg[...].astype(F32)] * heads, axis=1)
        spread = (spread * gain).astype(BF16)
        pick = (iota((width, hd), 0) % hd == iota((width, hd), 1)).astype(BF16)
        queries = mm(spread, pick)
        q_scr[...] = queries.astype(BF16)
        k_rows = jnp.broadcast_to(k.astype(F32)[:, None, :], (count, heads, hd)).reshape(rows, hd)
        own = jnp.sum(queries * k_rows, axis=1, keepdims=True) * scale
        own_scr[...] = jnp.broadcast_to(own, (rows, LANES))
        fv_scr[...] = jnp.broadcast_to(v.astype(F32)[:, None, :], (count, heads, hd)).reshape(rows, hd)
        local = jnp.where(second, fw[heads:, :].astype(F32), fw[:heads, :].astype(F32)).astype(BF16)
        bias = jnp.where(second, fb[:, heads:], fb[:, :heads])
        lf = jax.nn.log_sigmoid(mm_t(normed, local) + bias)
        lf = jnp.broadcast_to(lf[:, None, :], (count, heads, heads)).reshape(rows, heads)
        lf = jnp.where(iota((rows, heads), 1) == iota((rows, heads), 0) % heads, lf, 0.0)
        lf_scr[...] = jnp.broadcast_to(jnp.sum(lf, axis=1, keepdims=True), (rows, LANES))

    part = block * heads
    at = pl.ds(pl.multiple_of(step * part, part), part)
    queries = q_scr[at, :]
    scores = jnp.concatenate(
        [mm(queries[i * heads : (i + 1) * heads, :], key[i, 0]) for i in range(block)], axis=0
    )
    pos = iota((part, span), 1)
    length = jnp.concatenate(
        [jnp.full((heads, 1), len_ref[step * block + i], jnp.int32) for i in range(block)], axis=0
    )
    gates = gate[...].reshape(part, span)
    previous = jnp.sum(jnp.where(pos == length - 1, gates, 0.0), axis=1, keepdims=True)
    current = previous + lf_scr[at, :][:, :1]
    logits = jnp.where(pos < length, scores * scale + (current - gates), -jnp.inf)
    own = own_scr[at, :][:, :1]
    top = jnp.maximum(jnp.max(logits, axis=1, keepdims=True), own)
    weights = jnp.exp(logits - top)
    own_weight = jnp.exp(own - top)
    total = jnp.sum(weights, axis=1, keepdims=True) + own_weight
    probs = (weights / total).astype(BF16)
    own_prob = (own_weight / total).astype(BF16).astype(F32)
    mixed = jnp.concatenate(
        [mm_t(probs[i * heads : (i + 1) * heads, :], val[i, 0]) for i in range(block)], axis=0
    )
    mixed = mixed + own_prob * fv_scr[at, :]
    heads_scr[at, :] = mixed.astype(BF16).astype(F32)
    spot = iota((part, heads), 1) == iota((part, heads), 0) % heads
    cur = jnp.where(spot, current, 0.0).reshape(block, heads, heads)
    cur_out[pl.ds(pl.multiple_of(step * block, block), block), :] = jnp.sum(cur, axis=1)

    @pl.when(step == steps - 1)
    def _():
        pick = (iota((hd, width), 1) % hd == iota((hd, width), 0)).astype(BF16)
        wide = mm(heads_scr[...].astype(BF16), pick)
        mine = iota((rows, width), 1) // hd == iota((rows, width), 0) % heads
        wide = jnp.where(mine, wide, 0.0).reshape(count, heads, width)
        flat = jnp.sum(wide, axis=1).astype(BF16)
        partial[...] = mm(flat, ow[...]).astype(BF16)


def attend(lens, tok, ng, qw, kw, vw, fw, fb, qg, kg, key, val, gate, ow):
    count, heads, span = gate.shape
    hd = key.shape[2]
    width = tok.shape[1]
    block = 8
    steps = count // block
    rows = count * heads
    return pl.pallas_call(
        functools.partial(attend_kernel, block=block, steps=steps),
        grid_spec=pltpu.PrefetchScalarGridSpec(
            num_scalar_prefetch=1,
            grid=(steps,),
            in_specs=[
                whole(tok.shape), whole(ng.shape), whole(qw.shape), whole(kw.shape),
                whole(vw.shape), whole(fw.shape), whole(fb.shape), whole(qg.shape), whole(kg.shape),
                pl.BlockSpec((block, 1, hd, span), lambda i, *_: (i, 0, 0, 0)),
                pl.BlockSpec((block, 1, hd, span), lambda i, *_: (i, 0, 0, 0)),
                pl.BlockSpec((block, heads, span), lambda i, *_: (i, 0, 0)),
                whole(ow.shape),
            ],
            out_specs=[
                pl.BlockSpec(memory_space=pltpu.VMEM), whole((count, hd)), whole((count, hd)),
                whole((count, heads)),
            ],
            scratch_shapes=[
                pltpu.VMEM((rows, hd), BF16), pltpu.VMEM((rows, LANES), F32),
                pltpu.VMEM((rows, LANES), F32), pltpu.VMEM((rows, hd), F32),
                pltpu.VMEM((rows, hd), F32),
            ],
        ),
        out_shape=[
            jax.ShapeDtypeStruct((count, width), BF16), jax.ShapeDtypeStruct((count, hd), BF16),
            jax.ShapeDtypeStruct((count, hd), BF16), jax.ShapeDtypeStruct((count, heads), F32),
        ],
        compiler_params=params(60),
        name="attend",
    )(lens, tok, ng, qw, kw, vw, fw, fb, qg, kg, key, val, gate, ow)


def column(row, size):
    wide = jnp.broadcast_to(row, (size, size))
    return jnp.sum(jnp.where(iota((size, size), 0) == iota((size, size), 1), wide, 0), axis=1, keepdims=True)


def route_kernel(choice, info_out):
    count = choice.shape[1]
    picks = choice[...].astype(F32)
    earlier = iota((count, count), 1) < iota((count, count), 0)
    lane = iota((count, INFO), 1)
    info = jnp.zeros((count, INFO), F32)
    for k in range(SLOTS):
        mine_k = column(picks[k : k + 1, :], count)
        before = jnp.zeros((count, 1), F32)
        for other in range(SLOTS):
            same = jnp.logical_and(mine_k == picks[other : other + 1, :], earlier)
            before += jnp.sum(jnp.where(same, 1.0, 0.0), axis=1, keepdims=True)
        info = jnp.where(lane == k, mine_k * SLOTS + before, info)
    info_out[...] = info


def route(choice):
    out = jax.ShapeDtypeStruct((choice.shape[1], INFO), F32)
    return near_call(route_kernel, (choice,), out, limit=4)


def norm_kernel(tok, mine, theirs, pg, bg, info, copies, resid_out, branch_out):
    count, width = tok.shape
    half = width // 2
    second = lax.axis_index("tp") == 1
    attn = mine[...].astype(F32) + theirs[...].astype(F32)
    resid = (tok[...].astype(F32) + attn).astype(BF16).astype(F32)
    ms = jnp.mean(resid * resid, axis=1, keepdims=True)
    post = (resid * lax.rsqrt(ms + EPS) * laid_out(pg)).astype(BF16).astype(F32)
    line = jnp.concatenate(
        [jnp.where(second, post[:, half:], post[:, :half]), info[...]], axis=1
    ).astype(BF16)
    for peer in range(copies.shape[0]):
        copies[peer] = line
    logit = jnp.sum(post * laid_out(bg), axis=1, keepdims=True)
    branch_out[...] = jnp.broadcast_to(1.0 / (1.0 + jnp.exp(-logit)), (count, LANES))
    resid_out[...] = jnp.where(second, resid[:, half:], resid[:, :half])


def normalize(tok, mine, theirs, pg, bg, info, peers):
    count, width = tok.shape
    half = width // 2
    outs = [
        jax.ShapeDtypeStruct((peers, count, half + INFO), BF16),
        jax.ShapeDtypeStruct((count, half), F32),
        jax.ShapeDtypeStruct((count, LANES), F32),
    ]
    return near_call(norm_kernel, (tok, mine, theirs, pg, bg, info), outs, limit=8)


def hidden_kernel(x, *refs):
    (weights, (out, buf, sems)) = refs[:-3], refs[-3:]
    half, units = buf.shape[1:]
    rank = lax.axis_index("tp")
    moves = [
        pltpu.make_async_copy(
            w.at[pl.ds(pl.multiple_of(rank * half, half), half), :], buf.at[n], sems.at[n]
        )
        for n, w in enumerate(weights)
    ]
    for move in moves:
        move.start()
    tokens = x[:, :half]
    for b in range(len(weights) // 2):
        moves[2 * b].wait()
        moves[2 * b + 1].wait()
        w = jnp.concatenate([buf[2 * b], buf[2 * b + 1]], axis=1)
        out[:, 2 * units * b : 2 * units * (b + 1)] = mm(tokens, w).astype(BF16)


def dense_hidden(lines, weights):
    width, units = weights[0].shape
    here = pl.BlockSpec(memory_space=pltpu.VMEM)
    return pl.pallas_call(
        hidden_kernel,
        in_specs=[here] + [pl.BlockSpec(memory_space=pltpu.HBM)] * len(weights),
        out_specs=here,
        out_shape=jax.ShapeDtypeStruct((lines.shape[0], len(weights) * units), BF16),
        scratch_shapes=[
            pltpu.VMEM((len(weights), width // 2, units), BF16),
            pltpu.SemaphoreType.DMA((len(weights),)),
        ],
        compiler_params=params(16),
        name="dense_hidden",
    )(lines, *weights)


def extract_kernel(x, own_rows, near_rows, *, count):
    total = x.shape[0]
    half = own_rows.shape[1]
    peers = total // count
    shape = (total, 4 * peers)
    col = iota((1, 4 * peers), 1)
    expert = lax.axis_index("ep") ^ (col // (2 * peers))
    want = (expert * SLOTS + (col // peers) % 2).astype(F32)
    low = (col % peers) * count
    token = iota(shape, 0)
    info = x[:, half:].astype(F32)
    hit = jnp.logical_or(info[:, 0:1] == want, info[:, 1:2] == want)
    hit = jnp.logical_and(hit, jnp.logical_and(token >= low, token < low + count))
    pick = jnp.where(hit, 1.0, 0.0).astype(BF16)
    rows = lax.dot_general(
        pick, x[:, :half], (((0,), (0,)), ((), ())), preferred_element_type=F32
    ).astype(BF16)
    own_rows[...] = rows[: 2 * peers, :]
    near_rows[...] = rows[2 * peers :, :]


def extract(lines, count):
    total, wide = lines.shape
    rows = jax.ShapeDtypeStruct((2 * total // count, wide - INFO), BF16)
    kernel = functools.partial(extract_kernel, count=count)
    return near_call(kernel, (lines,), [rows, rows], limit=16)


def down_kernel(mine, theirs, *refs, count, block):
    weights, (far, squares, out, sems) = refs[:4], refs[4:]
    units = weights[0].shape[0]
    total, half = out.shape
    moves = []
    peers = total // count
    w = jnp.concatenate([kept(a, 1, half) for a in weights], axis=0)
    part = jnp.zeros((peers, LANES), F32)
    for step in range(total // block):
        at = slice(step * block, (step + 1) * block)

        def full(b):
            there = b ^ 1
            return mine[at, b * units : (b + 1) * units].astype(F32) + theirs[
                at, there * units : (there + 1) * units
            ].astype(F32)

        hidden = [silu(full(b)) * full(b + 2) for b in (0, 1, 4, 5)]
        square = jnp.sum(sum(h * h for h in hidden), axis=1, keepdims=True)
        h = jnp.concatenate([a.astype(BF16) for a in hidden], axis=1)
        out[at, :] = mm(h, w).astype(BF16)
        moves.append(pltpu.make_async_copy(out.at[at, :], far.at[at, :], sems.at[step]))
        moves[-1].start()
        token = iota((block, LANES), 0) + step * block
        spread = jnp.where(iota((block, LANES), 1) == token % count, square, 0.0)
        high = spread.astype(BF16)
        low = (spread - high.astype(F32)).astype(BF16)
        here = iota((peers, block), 1) + step * block
        start = iota((peers, block), 0) * count
        owner = jnp.logical_and(here >= start, here < start + count)
        owner = jnp.where(owner, 1.0, 0.0).astype(BF16)
        part += mm(owner, high) + mm(owner, low)
    squares[...] = part
    for move in moves:
        move.wait()


def dense_down(mine, theirs, weights, count):
    total = mine.shape[0]
    half = weights[0].shape[1] // 2
    block = 256
    here = pl.BlockSpec(memory_space=pltpu.VMEM)
    return pl.pallas_call(
        functools.partial(down_kernel, count=count, block=block),
        in_specs=[here] * (2 + len(weights)),
        out_specs=[pl.BlockSpec(memory_space=pltpu.HBM), here],
        out_shape=[
            jax.ShapeDtypeStruct((total, half), BF16),
            jax.ShapeDtypeStruct((total // count, LANES), F32),
        ],
        scratch_shapes=[
            pltpu.VMEM((total, half), BF16), pltpu.SemaphoreType.DMA((total // block,)),
        ],
        compiler_params=params(16),
        name="dense_down",
    )(mine, theirs, *weights)


def expert_kernel(a0, b0, a1, b1, gw, uw, dw, after, keep, give, gbuf, ubuf, dbuf, sems):
    half = a0.shape[1]
    moves = []
    for n, (far, buf) in enumerate(((gw, gbuf), (uw, ubuf), (dw, dbuf))):
        part = buf.shape[0] // 2
        for m in range(2):
            at = pl.ds(m * part, part)
            moves.append(pltpu.make_async_copy(far.at[0, at, :], buf.at[at, :], sems.at[2 * n + m]))
            moves[-1].start()
    x0 = jnp.concatenate([a0[...], b0[...]], axis=0)
    x1 = jnp.concatenate([a1[...], b1[...]], axis=0)

    def rows(w):
        return mm(x0, kept(w, 0, half)) + mm(x1, kept(w, 0, half, True))

    moves[0].wait()
    moves[1].wait()
    gate = silu(rows(gbuf))
    moves[2].wait()
    moves[3].wait()
    act = (gate * rows(ubuf)).astype(BF16)
    moves[4].wait()
    moves[5].wait()
    keep[...] = mm(act, kept(dbuf, 1, half)).astype(BF16)
    give[...] = mm(act, kept(dbuf, 1, half, True)).astype(BF16)


def experts(rows, away, gate_w, up_w, down_w, after):
    count, half = rows[0].shape
    here = pl.BlockSpec(memory_space=pltpu.VMEM)
    far = pl.BlockSpec(memory_space=pltpu.HBM)
    return pl.pallas_call(
        expert_kernel,
        in_specs=[here] * 4 + [far] * 3 + [here],
        out_specs=[here] * 2,
        out_shape=[jax.ShapeDtypeStruct((2 * count, half), BF16)] * 2,
        scratch_shapes=[pltpu.VMEM(w.shape[1:], BF16) for w in (gate_w, up_w, down_w)]
        + [pltpu.SemaphoreType.DMA((6,))],
        compiler_params=params(24),
        name="experts",
    )(*rows, *away, gate_w, up_w, down_w, after)


def answer_kernel(keep, other, squares, out, scr):
    mine = class_of(lax.axis_index("ep"))
    peers = out.shape[0]
    total = keep[...].astype(F32) + other[...].astype(F32)
    parts = total.shape[1] // LANES
    for q in range(2):
        for s in range(SLOTS):
            own = total[peers * s : peers * (s + 1), :]
            near = total[2 * peers + peers * s : 2 * peers + peers * (s + 1), :]
            rows = jnp.where((iota((peers, 1), 0) + q) % 2 == mine, own, near)
            for f in range(parts):
                scr[:, parts * s + f, :] = rows[:, LANES * f : LANES * (f + 1)]
        out[:, q, : SLOTS * parts, :] = scr[...].astype(BF16)
        line = jnp.where((iota((peers, 1), 0) + q) % 2 == mine, squares[...], 0.0)
        out[:, q, SLOTS * parts :, :] = jnp.broadcast_to(line[:, None, :], (peers, 8, LANES)).astype(BF16)


def answers(keep, other, squares):
    peers = squares.shape[0]
    half = keep.shape[1]
    rows = SLOTS * half // LANES
    out = jax.ShapeDtypeStruct((peers, 2, rows + 8, LANES), BF16)
    scratch = [pltpu.VMEM((peers, rows, LANES), F32)]
    return near_call(answer_kernel, (keep, other, squares), out, scratch, limit=16)


def last_kernel(returned, parts, info, weight, branch, resid, out, scr):
    count, half = resid.shape
    ep = returned.shape[0]
    tiles = half // LANES
    rows = SLOTS * tiles
    scr[...] = returned[:, :rows, :].astype(F32)
    values = jnp.concatenate(
        [
            jnp.concatenate([scr[:, tiles * s + f, :] for f in range(tiles)], axis=1)
            for s in range(SLOTS)
        ],
        axis=0,
    ).astype(BF16)
    lane = iota((count, SLOTS * ep), 1)
    code = ((lane % ep) * SLOTS + lane // ep).astype(F32)
    expert_sum = jnp.zeros((count, half), F32)
    for k in range(SLOTS):
        pick = jnp.where(info[:, k : k + 1] == code, 1.0, 0.0).astype(BF16)
        expert_sum += column(weight[k : k + 1, :], count) * mm(pick, values)
    square = jnp.sum(returned[:, rows : rows + 8, :].astype(F32), axis=0)
    square = column(square[0:1, :count], count)
    dense = jnp.sum(parts[...].astype(F32), axis=0)
    dense = (dense * lax.rsqrt(square / FF2 + EPS)).astype(BF16).astype(F32)
    out[...] = (resid[...] + expert_sum + branch[:, :1] * dense).astype(BF16)


def last_sum(returned, parts, info, weight, branch, resid):
    arrays = (returned, parts, info, weight, branch, resid)
    out = jax.ShapeDtypeStruct(resid.shape, BF16)
    scratch = [pltpu.VMEM((returned.shape[0], SLOTS * resid.shape[1] // LANES, LANES), F32)]
    return near_call(last_kernel, arrays, out, scratch, limit=16)


def body(
    tokens,
    norm_gain,
    query_w,
    key_w,
    value_w,
    forget_w,
    forget_bias,
    query_gain,
    key_gain,
    cache_key,
    cache_value,
    cache_gate,
    cache_len,
    out_w,
    post_gain,
    branch_gate,
    dense_gate_w,
    dense_up_w,
    dense_down_w,
    expert_choice,
    route_weight,
    expert_gate_w,
    expert_up_w,
    expert_down_w,
):
    count = tokens.shape[0]
    ep_count = lax.axis_size("ep")
    peers = ep_count // 2
    pair = [(e, e ^ 1) for e in range(ep_count)]
    classes = [[e for e in range(ep_count) if class_of(e) == c] for c in range(2)]

    near = []
    for array in (dense_gate_w, dense_up_w, dense_down_w):
        near.append(lax.ppermute(array, "ep", pair))

    partial, fresh_key, fresh_value, current = attend(
        cache_len, tokens, tiled(norm_gain), query_w, key_w, value_w, forget_w.T,
        forget_bias[None], query_gain[None], key_gain[None], cache_key, cache_value,
        cache_gate, out_w,
    )
    partial_other = swapped(partial)
    info = route(expert_choice.T)
    copies, resid, branch = normalize(
        tokens, partial, partial_other, tiled(post_gain), tiled(branch_gate), info, peers
    )
    lines = lax.all_to_all(copies, "ep", 0, 0, tiled=True, axis_index_groups=classes)
    lines = lines.reshape(peers * count, -1)

    gate_up = []
    for gate_w, up_w in ((dense_gate_w, dense_up_w), (near[0], near[1])):
        gate_up += [gate_w, swapped(gate_w), up_w, swapped(up_w)]
    downs = []
    for down_w in (dense_down_w, near[2]):
        downs += [down_w, swapped(down_w)]

    part = dense_hidden(lines, gate_up)
    part_other = swapped(part)
    own_rows, near_rows = extract(lines, count)
    pair_rows = lax.ppermute(near_rows, "ep", pair)
    terms, squares = dense_down(part, part_other, downs, count)
    parts = lax.all_to_all(
        terms.reshape(peers, count, -1), "ep", 0, 0, tiled=True, axis_index_groups=classes
    )

    away = (swapped(own_rows), swapped(pair_rows))
    keep, give = experts(
        (own_rows, pair_rows), away, expert_gate_w, expert_up_w, expert_down_w, squares
    )
    answer = answers(keep, swapped(give), squares)
    returned = lax.all_to_all(answer.reshape(ep_count, *answer.shape[2:]), "ep", 0, 0, tiled=True)
    mixed_out = last_sum(returned, parts, info, route_weight.T, branch, resid)
    return (mixed_out, fresh_key[:, None, :], fresh_value[:, None, :], current)


def solution(mesh):
    placed = (
        P("ep", None),
        P(),
        P(None, "tp"),
        P(),
        P(),
        P(),
        P(),
        P(),
        P(),
        P("ep", "tp", None, None),
        P("ep", "tp", None, None),
        P("ep", "tp", None),
        P("ep"),
        P("tp", None),
        P(),
        P(),
        P(None, ("ep", "tp")),
        P(None, ("ep", "tp")),
        P(("ep", "tp"), None),
        P("ep", None),
        P("ep", None),
        P("ep", None, "tp"),
        P("ep", None, "tp"),
        P("ep", "tp", None),
    )

    return jax.shard_map(
        body,
        mesh=mesh,
        in_specs=placed,
        out_specs=(P("ep", "tp"), P("ep", "tp", None), P("ep", "tp", None), P("ep", "tp")),
        check_vma=False,
    )
```

```python
import functools

import jax
import jax.numpy as jnp
from jax import lax
from jax.experimental import pallas as pl
from jax.experimental.pallas import tpu as pltpu
from jax.sharding import PartitionSpec as P


FF2 = 16384
LANES = 128
INFO = 128
SLOTS = 2
EPS = 1e-06
SWAP = [(0, 1), (1, 0)]
F32 = jnp.float32
BF16 = jnp.bfloat16


def class_of(e):
    return (e ^ (e // 2)) % 2


def swapped(array):
    return lax.ppermute(array, "tp", SWAP)


def iota(shape, dim):
    return lax.broadcasted_iota(jnp.int32, shape, dim)


def mm(a, b):
    return jnp.dot(a, b, preferred_element_type=F32)


def mm_t(a, b):
    return lax.dot_general(a, b, (((1,), (1,)), ((), ())), preferred_element_type=F32)


def silu(v):
    return v / (1.0 + jnp.exp(-v))


def params(limit=56):
    return pltpu.CompilerParams(vmem_limit_bytes=limit << 20)


def whole(shape):
    return pl.BlockSpec(shape, lambda *_: (0,) * len(shape))


def near_call(kernel, arrays, outs, scratch=(), limit=32):
    here = pl.BlockSpec(memory_space=pltpu.VMEM)
    many = isinstance(outs, list)
    return pl.pallas_call(
        kernel,
        in_specs=[here] * len(arrays),
        out_specs=[here] * len(outs) if many else here,
        out_shape=outs,
        scratch_shapes=list(scratch),
        compiler_params=params(limit),
    )(*arrays)


def kept(ref, dim, size, other=False):
    rank = lax.axis_index("tp")
    rank = 1 - rank if other else rank
    at = pl.ds(pl.multiple_of(rank * size, size), size)
    return ref[at, :] if dim == 0 else ref[:, at]


def laid_out(ref):
    rows = ref[...].astype(F32)
    return jnp.concatenate([rows[r : r + 1, :] for r in range(rows.shape[0])], axis=1)


def tiled(vector):
    return vector.reshape(-1, LANES)


def attend_kernel(
    len_ref, fb, qg, kg, tok_f, ng_f, qw_f, kw_f, vw_f, fw_f, key_f, val_f, gate_f, ow_f,
    partial, fk_out, fv_out, cur_out,
    tok, ng, qw, kw, vw, fw, key, val, gate, ow, sems, *, block,
):
    count = tok.shape[0]
    heads = gate.shape[1]
    hd = key.shape[2]
    span = key.shape[3]
    rows = count * heads
    width = heads * hd
    scale = hd ** (-0.5)
    second = lax.axis_index("tp") == 1
    moves = []

    def fetch(far, buf):
        moves.append(pltpu.make_async_copy(far, buf, sems.at[len(moves)]))
        moves[-1].start()
        return moves[-1]

    first = [fetch(f, v) for f, v in ((tok_f, tok), (ng_f, ng))]
    loads = [fetch(f, v) for f, v in ((qw_f, qw), (kw_f, kw), (vw_f, vw), (fw_f, fw))]
    pieces = [pl.ds(at, block) for at in range(0, count, block)]
    key_moves = [fetch(key_f.at[at], key.at[at]) for at in pieces]
    gate_move = fetch(gate_f, gate)
    val_moves = [fetch(val_f.at[at], val.at[at]) for at in pieces]
    out_load = fetch(ow_f, ow)

    for move in first:
        move.wait()
    x = tok[...].astype(F32)
    ms = jnp.mean(x * x, axis=1, keepdims=True)
    normed = (x * lax.rsqrt(ms + EPS) * laid_out(ng)).astype(BF16)
    for move in loads:
        move.wait()
    q = mm(normed, qw[...])
    k = mm(normed, kw[...])
    v = mm(normed, vw[...])
    k = jnp.where(second, k[:, hd:], k[:, :hd])
    v = jnp.where(second, v[:, hd:], v[:, :hd]).astype(BF16)
    k = k * lax.rsqrt(jnp.mean(k * k, axis=1, keepdims=True) + EPS) * kg[...].astype(F32)
    k = k.astype(BF16)
    fk_out[...] = k
    fv_out[...] = v
    spread = jnp.broadcast_to(q[:, None, :], (count, heads, width)).reshape(rows, width)
    mine = iota((rows, width), 1) // hd == iota((rows, width), 0) % heads
    spread = jnp.where(mine, spread, 0.0)
    msq = jnp.sum(spread * spread, axis=1, keepdims=True) / hd
    spread = spread * lax.rsqrt(msq + EPS)
    gain = jnp.concatenate([qg[...].astype(F32)] * heads, axis=1)
    spread = (spread * gain).astype(BF16)
    pick = (iota((width, hd), 0) % hd == iota((width, hd), 1)).astype(BF16)
    queries_f = mm(spread, pick)
    queries = queries_f.astype(BF16)
    k_rows = jnp.broadcast_to(k.astype(F32)[:, None, :], (count, heads, hd)).reshape(rows, hd)
    own_all = jnp.sum(queries_f * k_rows, axis=1, keepdims=True) * scale
    v_rows = jnp.broadcast_to(v.astype(F32)[:, None, :], (count, heads, hd)).reshape(rows, hd)
    local = jnp.where(second, fw[heads:, :].astype(F32), fw[:heads, :].astype(F32)).astype(BF16)
    bias = jnp.where(second, fb[:, heads:], fb[:, :heads])
    lf = jax.nn.log_sigmoid(mm_t(normed, local) + bias)
    lf = jnp.broadcast_to(lf[:, None, :], (count, heads, heads)).reshape(rows, heads)
    lf = jnp.where(iota((rows, heads), 1) == iota((rows, heads), 0) % heads, lf, 0.0)
    lf_all = jnp.sum(lf, axis=1, keepdims=True)

    pos = iota((rows, span), 1)
    spot = iota((rows, heads), 1) == iota((rows, heads), 0) % heads
    length = jnp.concatenate(
        [jnp.full((heads, 1), len_ref[i], jnp.int32) for i in range(count)], axis=0
    )
    scores = []
    for i in range(count):
        if i % block == 0:
            key_moves[i // block].wait()
        scores.append(mm(queries[i * heads : (i + 1) * heads], key[i, 0]))
    scores = jnp.concatenate(scores, axis=0)
    gate_move.wait()
    gates = gate[...].reshape(rows, span)
    previous = jnp.sum(jnp.where(pos == length - 1, gates, 0.0), axis=1, keepdims=True)
    current = previous + lf_all
    logits = jnp.where(pos < length, scores * scale + (current - gates), -jnp.inf)
    top = jnp.maximum(jnp.max(logits, axis=1, keepdims=True), own_all)
    weights = jnp.exp(logits - top)
    own_weight = jnp.exp(own_all - top)
    total = jnp.sum(weights, axis=1, keepdims=True) + own_weight
    probs = (weights / total).astype(BF16)
    own_prob = (own_weight / total).astype(BF16).astype(F32)
    mixed = []
    for i in range(count):
        if i % block == 0:
            val_moves[i // block].wait()
        mixed.append(mm_t(probs[i * heads : (i + 1) * heads], val[i, 0]))
    mixed = jnp.concatenate(mixed, axis=0) + own_prob * v_rows
    cur = jnp.where(spot, current, 0.0).reshape(count, heads, heads)
    cur_out[...] = jnp.sum(cur, axis=1)

    pick = (iota((hd, width), 1) % hd == iota((hd, width), 0)).astype(BF16)
    wide = mm(mixed.astype(BF16), pick)
    wide = jnp.where(mine, wide, 0.0).reshape(count, heads, width)
    flat = jnp.sum(wide, axis=1).astype(BF16)
    out_load.wait()
    partial[...] = mm(flat, ow[...]).astype(BF16)


def attend(lens, tok, ng, qw, kw, vw, fw, fb, qg, kg, key, val, gate, ow):
    count, heads, _ = gate.shape
    hd = key.shape[2]
    width = tok.shape[1]
    block = 8
    big = (tok, ng, qw, kw, vw, fw, key, val, gate, ow)
    far = pl.BlockSpec(memory_space=pltpu.HBM)
    return pl.pallas_call(
        functools.partial(attend_kernel, block=block),
        grid_spec=pltpu.PrefetchScalarGridSpec(
            num_scalar_prefetch=1,
            grid=(1,),
            in_specs=[whole(fb.shape), whole(qg.shape), whole(kg.shape)] + [far] * len(big),
            out_specs=[
                whole((count, width)), whole((count, hd)), whole((count, hd)), whole((count, heads)),
            ],
            scratch_shapes=[pltpu.VMEM(a.shape, a.dtype) for a in big]
            + [
                pltpu.SemaphoreType.DMA((8 + 2 * (count // block),)),
            ],
        ),
        out_shape=[
            jax.ShapeDtypeStruct((count, width), BF16), jax.ShapeDtypeStruct((count, hd), BF16),
            jax.ShapeDtypeStruct((count, hd), BF16), jax.ShapeDtypeStruct((count, heads), F32),
        ],
        compiler_params=params(60),
        name="attend",
    )(lens, fb, qg, kg, *big)


def column(row, size):
    wide = jnp.broadcast_to(row, (size, size))
    return jnp.sum(jnp.where(iota((size, size), 0) == iota((size, size), 1), wide, 0), axis=1, keepdims=True)


def route_kernel(choice, info_out):
    count = choice.shape[1]
    picks = choice[...].astype(F32)
    earlier = iota((count, count), 1) < iota((count, count), 0)
    lane = iota((count, INFO), 1)
    info = jnp.zeros((count, INFO), F32)
    for k in range(SLOTS):
        mine_k = column(picks[k : k + 1, :], count)
        before = jnp.zeros((count, 1), F32)
        for other in range(SLOTS):
            same = jnp.logical_and(mine_k == picks[other : other + 1, :], earlier)
            before += jnp.sum(jnp.where(same, 1.0, 0.0), axis=1, keepdims=True)
        info = jnp.where(lane == k, mine_k * SLOTS + before, info)
    info_out[...] = info


def route(choice):
    out = jax.ShapeDtypeStruct((choice.shape[1], INFO), F32)
    return near_call(route_kernel, (choice,), out, limit=4)


def norm_kernel(tok, mine, theirs, pg, bg, info, copies, resid_out, branch_out):
    count, width = tok.shape
    half = width // 2
    second = lax.axis_index("tp") == 1
    attn = mine[...].astype(F32) + theirs[...].astype(F32)
    resid = (tok[...].astype(F32) + attn).astype(BF16).astype(F32)
    ms = jnp.mean(resid * resid, axis=1, keepdims=True)
    post = (resid * lax.rsqrt(ms + EPS) * laid_out(pg)).astype(BF16).astype(F32)
    line = jnp.concatenate(
        [jnp.where(second, post[:, half:], post[:, :half]), info[...]], axis=1
    ).astype(BF16)
    for peer in range(copies.shape[0]):
        copies[peer] = line
    logit = jnp.sum(post * laid_out(bg), axis=1, keepdims=True)
    branch_out[...] = jnp.broadcast_to(1.0 / (1.0 + jnp.exp(-logit)), (count, LANES))
    resid_out[...] = jnp.where(second, resid[:, half:], resid[:, :half]).astype(BF16)


def normalize(tok, mine, theirs, pg, bg, info, peers):
    count, width = tok.shape
    half = width // 2
    outs = [
        jax.ShapeDtypeStruct((peers, count, half + INFO), BF16),
        jax.ShapeDtypeStruct((count, half), BF16),
        jax.ShapeDtypeStruct((count, LANES), F32),
    ]
    return near_call(norm_kernel, (tok, mine, theirs, pg, bg, info), outs, limit=8)


def pack_kernel(*refs):
    weights, (out, sems) = refs[:-2], refs[-2:]
    half = out.shape[0]
    units = weights[0].shape[1]
    at = pl.ds(pl.multiple_of(lax.axis_index("tp") * half, half), half)
    moves = [
        pltpu.make_async_copy(w.at[at, :], out.at[:, pl.ds(n * units, units)], sems.at[n])
        for n, w in enumerate(weights)
    ]
    for move in moves:
        move.start()
    for move in moves:
        move.wait()


def pack_down_kernel(*refs):
    weights, (out, sems) = refs[:-2], refs[-2:]
    half = out.shape[1]
    units = weights[0].shape[0]
    at = pl.ds(pl.multiple_of(lax.axis_index("tp") * half, half), half)
    moves = [
        pltpu.make_async_copy(w.at[:, at], out.at[pl.ds(n * units, units), :], sems.at[n])
        for n, w in enumerate(weights)
    ]
    for move in moves:
        move.start()
    for move in moves:
        move.wait()


def pack(kernel, weights, shape):
    return pl.pallas_call(
        kernel,
        in_specs=[pl.BlockSpec(memory_space=pltpu.HBM)] * len(weights),
        out_specs=pl.BlockSpec(memory_space=pltpu.VMEM),
        out_shape=jax.ShapeDtypeStruct(shape, BF16),
        scratch_shapes=[pltpu.SemaphoreType.DMA((len(weights),))],
        compiler_params=params(16),
    )(*weights)


def hidden_kernel(x, wide, out):
    half = wide.shape[0]
    tokens = x[:, :half]
    for b in range(wide.shape[1] // 256):
        at = slice(256 * b, 256 * (b + 1))
        out[:, at] = mm(tokens, wide[:, at]).astype(BF16)


def dense_hidden(lines, wide):
    out = jax.ShapeDtypeStruct((lines.shape[0], wide.shape[1]), BF16)
    return near_call(hidden_kernel, (lines, wide), out, limit=16)


def extract_kernel(x, own_rows, near_rows, *, count):
    total = x.shape[0]
    half = own_rows.shape[1]
    peers = total // count
    shape = (total, 4 * peers)
    col = iota((1, 4 * peers), 1)
    expert = lax.axis_index("ep") ^ (col // (2 * peers))
    want = (expert * SLOTS + (col // peers) % 2).astype(F32)
    low = (col % peers) * count
    token = iota(shape, 0)
    info = x[:, half:].astype(F32)
    hit = jnp.logical_or(info[:, 0:1] == want, info[:, 1:2] == want)
    hit = jnp.logical_and(hit, jnp.logical_and(token >= low, token < low + count))
    pick = jnp.where(hit, 1.0, 0.0).astype(BF16)
    rows = lax.dot_general(
        pick, x[:, :half], (((0,), (0,)), ((), ())), preferred_element_type=F32
    ).astype(BF16)
    own_rows[...] = rows[: 2 * peers, :]
    near_rows[...] = rows[2 * peers :, :]


def extract(lines, count):
    total, wide = lines.shape
    rows = jax.ShapeDtypeStruct((2 * total // count, wide - INFO), BF16)
    kernel = functools.partial(extract_kernel, count=count)
    return near_call(kernel, (lines,), [rows, rows], limit=16)


def down_kernel(mine, theirs, down, far, squares_far, out, hid, squares, sems, *, count, block):
    units = mine.shape[1] // 8
    total, _ = out.shape
    peers = total // count
    steps = [slice(at, at + block) for at in range(0, total, block)]
    part = jnp.zeros((peers, LANES), F32)
    for at in steps:

        def full(b):
            there = b ^ 1
            return mine[at, b * units : (b + 1) * units].astype(F32) + theirs[
                at, there * units : (there + 1) * units
            ].astype(F32)

        hidden = [silu(full(b)) * full(b + 2) for b in (0, 1, 4, 5)]
        square = jnp.sum(sum(h * h for h in hidden), axis=1, keepdims=True)
        hid[at, :] = jnp.concatenate([a.astype(BF16) for a in hidden], axis=1)
        token = iota((block, LANES), 0) + at.start
        spread = jnp.where(iota((block, LANES), 1) == token % count, square, 0.0)
        high = spread.astype(BF16)
        low = (spread - high.astype(F32)).astype(BF16)
        here = iota((peers, block), 1) + at.start
        start = iota((peers, block), 0) * count
        owner = jnp.logical_and(here >= start, here < start + count)
        owner = jnp.where(owner, 1.0, 0.0).astype(BF16)
        part += mm(owner, high) + mm(owner, low)
    squares[...] = part
    moves = [pltpu.make_async_copy(squares, squares_far, sems.at[0])]
    moves[0].start()
    for n, at in enumerate(steps):
        out[at, :] = mm(hid[at, :], down[...]).astype(BF16)
        moves.append(pltpu.make_async_copy(out.at[at, :], far.at[at, :], sems.at[n + 1]))
        moves[-1].start()
    for move in moves:
        move.wait()


def dense_down(mine, theirs, down, count):
    total = mine.shape[0]
    units, half = down.shape
    block = 256
    here = pl.BlockSpec(memory_space=pltpu.VMEM)
    far = pl.BlockSpec(memory_space=pltpu.HBM)
    return pl.pallas_call(
        functools.partial(down_kernel, count=count, block=block),
        in_specs=[here] * 3,
        out_specs=[far, far],
        out_shape=[
            jax.ShapeDtypeStruct((total, half), BF16),
            jax.ShapeDtypeStruct((total // count, LANES), F32),
        ],
        scratch_shapes=[
            pltpu.VMEM((total, half), BF16), pltpu.VMEM((total, units), BF16),
            pltpu.VMEM((total // count, LANES), F32),
            pltpu.SemaphoreType.DMA((total // block + 1,)),
        ],
        compiler_params=params(16),
        name="dense_down",
    )(mine, theirs, down)


def expert_kernel(a0, b0, a1, b1, gw, uw, dw, after, keep, give, gbuf, ubuf, dbuf, sems):
    half = a0.shape[1]
    moves = []
    for n, (far, buf) in enumerate(((gw, gbuf), (uw, ubuf), (dw, dbuf))):
        part = buf.shape[0] // 2
        for m in range(2):
            at = pl.ds(m * part, part)
            moves.append(pltpu.make_async_copy(far.at[0, at, :], buf.at[at, :], sems.at[2 * n + m]))
            moves[-1].start()
    x0 = jnp.concatenate([a0[...], b0[...]], axis=0)
    x1 = jnp.concatenate([a1[...], b1[...]], axis=0)

    def rows(w):
        return mm(x0, kept(w, 0, half)) + mm(x1, kept(w, 0, half, True))

    moves[0].wait()
    moves[1].wait()
    gate = silu(rows(gbuf))
    moves[2].wait()
    moves[3].wait()
    act = (gate * rows(ubuf)).astype(BF16)
    moves[4].wait()
    moves[5].wait()
    keep[...] = mm(act, kept(dbuf, 1, half)).astype(BF16)
    give[...] = mm(act, kept(dbuf, 1, half, True)).astype(BF16)


def experts(rows, away, gate_w, up_w, down_w, after):
    count, half = rows[0].shape
    here = pl.BlockSpec(memory_space=pltpu.VMEM)
    far = pl.BlockSpec(memory_space=pltpu.HBM)
    return pl.pallas_call(
        expert_kernel,
        in_specs=[here] * 4 + [far] * 3 + [here],
        out_specs=[here] * 2,
        out_shape=[jax.ShapeDtypeStruct((2 * count, half), BF16)] * 2,
        scratch_shapes=[pltpu.VMEM(w.shape[1:], BF16) for w in (gate_w, up_w, down_w)]
        + [pltpu.SemaphoreType.DMA((6,))],
        compiler_params=params(60),
        name="experts",
    )(*rows, *away, gate_w, up_w, down_w, after)


def merge_kernel(keep, other, near):
    half = near.shape[0]
    near[...] = (keep[half:, :].astype(F32) + other[half:, :].astype(F32)).astype(BF16)


def merge(keep, other):
    out = jax.ShapeDtypeStruct((keep.shape[0] // 2, keep.shape[1]), BF16)
    return near_call(merge_kernel, (keep, other), out, limit=16)


def answer_kernel(keep, other, near, squares, out, scr):
    peers = out.shape[0]
    half = near.shape[0]
    own = keep[:half, :].astype(F32) + other[:half, :].astype(F32)
    parts = own.shape[1] // LANES
    for g, total in enumerate((own, near[...].astype(F32))):
        for s in range(SLOTS):
            for f in range(parts):
                scr[:, parts * (SLOTS * g + s) + f, :] = total[
                    peers * s : peers * (s + 1), LANES * f : LANES * (f + 1)
                ]
    out[:, : 2 * SLOTS * parts, :] = scr[...].astype(BF16)
    out[:, 2 * SLOTS * parts :, :] = jnp.broadcast_to(
        squares[...][:, None, :], (peers, 8, LANES)
    ).astype(BF16)


def answers(keep, other, near, squares):
    peers = squares.shape[0]
    rows = 2 * SLOTS * keep.shape[1] // LANES
    out = jax.ShapeDtypeStruct((peers, rows + 8, LANES), BF16)
    scratch = [pltpu.VMEM((peers, rows, LANES), F32)]
    return near_call(answer_kernel, (keep, other, near, squares), out, scratch, limit=16)


def last_kernel(returned, parts, info, weight, branch, resid, out, scr):
    count, half = resid.shape
    peers = returned.shape[0]
    tiles = half // LANES
    rows = 2 * SLOTS * tiles
    scr[...] = returned[:, :rows, :].astype(F32)
    values = jnp.concatenate(
        [
            jnp.concatenate([scr[:, tiles * b + f, :] for f in range(tiles)], axis=1)
            for b in range(2 * SLOTS)
        ],
        axis=0,
    ).astype(BF16)
    lane = iota((1, 2 * SLOTS * peers), 1)
    peer = lane % peers
    expert = (2 * peer + (peer + class_of(lax.axis_index("ep"))) % 2) ^ (lane // (SLOTS * peers))
    code = (expert * SLOTS + (lane // peers) % SLOTS).astype(F32)
    expert_sum = jnp.zeros((count, half), F32)
    for k in range(SLOTS):
        pick = jnp.where(info[:, k : k + 1] == code, 1.0, 0.0).astype(BF16)
        expert_sum += column(weight[k : k + 1, :], count) * mm(pick, values)
    square = jnp.sum(returned[:, rows : rows + 8, :].astype(F32), axis=0)
    square = column(square[0:1, :count], count)
    dense = jnp.sum(parts[...].astype(F32), axis=0)
    dense = (dense * lax.rsqrt(square / FF2 + EPS)).astype(BF16).astype(F32)
    out[...] = (resid[...].astype(F32) + expert_sum + branch[:, :1] * dense).astype(BF16)


def last_sum(returned, parts, info, weight, branch, resid):
    arrays = (returned, parts, info, weight, branch, resid)
    out = jax.ShapeDtypeStruct(resid.shape, BF16)
    scratch = [pltpu.VMEM((returned.shape[0], 2 * SLOTS * resid.shape[1] // LANES, LANES), F32)]
    return near_call(last_kernel, arrays, out, scratch, limit=16)


def body(
    tokens,
    norm_gain,
    query_w,
    key_w,
    value_w,
    forget_w,
    forget_bias,
    query_gain,
    key_gain,
    cache_key,
    cache_value,
    cache_gate,
    cache_len,
    out_w,
    post_gain,
    branch_gate,
    dense_gate_w,
    dense_up_w,
    dense_down_w,
    expert_choice,
    route_weight,
    expert_gate_w,
    expert_up_w,
    expert_down_w,
):
    count = tokens.shape[0]
    ep_count = lax.axis_size("ep")
    peers = ep_count // 2
    pair = [(e, e ^ 1) for e in range(ep_count)]
    classes = [[e for e in range(ep_count) if class_of(e) == c] for c in range(2)]

    near = []
    for array in (dense_gate_w, dense_up_w, dense_down_w):
        near.append(lax.ppermute(array, "ep", pair))

    partial, fresh_key, fresh_value, current = attend(
        cache_len, tokens, tiled(norm_gain), query_w, key_w, value_w, forget_w.T,
        forget_bias[None], query_gain[None], key_gain[None], cache_key, cache_value,
        cache_gate, out_w,
    )
    partial_other = swapped(partial)
    info = route(expert_choice.T)
    copies, resid, branch = normalize(
        tokens, partial, partial_other, tiled(post_gain), tiled(branch_gate), info, peers
    )
    lines = lax.all_to_all(copies, "ep", 0, 0, tiled=True, axis_index_groups=classes)
    lines = lines.reshape(peers * count, -1)

    gate_up = []
    for gate_w, up_w in ((dense_gate_w, dense_up_w), (near[0], near[1])):
        gate_up += [gate_w, swapped(gate_w), up_w, swapped(up_w)]
    downs = []
    for down_w in (dense_down_w, near[2]):
        downs += [down_w, swapped(down_w)]

    width, units = dense_gate_w.shape
    wide = pack(pack_kernel, gate_up, (width // 2, len(gate_up) * units))
    down = pack(pack_down_kernel, downs, (len(downs) * units, width // 2))
    part = dense_hidden(lines, wide)
    part_other = swapped(part)
    own_rows, near_rows = extract(lines, count)
    pair_rows = lax.ppermute(near_rows, "ep", pair)
    terms, squares = dense_down(part, part_other, down, count)
    parts = lax.all_to_all(
        terms.reshape(peers, count, -1), "ep", 0, 0, tiled=True, axis_index_groups=classes
    )

    away = (swapped(own_rows), swapped(pair_rows))
    keep, give = experts(
        (own_rows, pair_rows), away, expert_gate_w, expert_up_w, expert_down_w, squares
    )
    other = swapped(give)
    back = lax.ppermute(merge(keep, other), "ep", pair)
    answer = answers(keep, other, back, squares)
    returned = lax.all_to_all(answer, "ep", 0, 0, tiled=True, axis_index_groups=classes)
    mixed_out = last_sum(returned, parts, info, route_weight.T, branch, resid)
    return (mixed_out, fresh_key[:, None, :], fresh_value[:, None, :], current)


def solution(mesh):
    placed = (
        P("ep", None),
        P(),
        P(None, "tp"),
        P(),
        P(),
        P(),
        P(),
        P(),
        P(),
        P("ep", "tp", None, None),
        P("ep", "tp", None, None),
        P("ep", "tp", None),
        P("ep"),
        P("tp", None),
        P(),
        P(),
        P(None, ("ep", "tp")),
        P(None, ("ep", "tp")),
        P(("ep", "tp"), None),
        P("ep", None),
        P("ep", None),
        P("ep", None, "tp"),
        P("ep", None, "tp"),
        P("ep", "tp", None),
    )

    return jax.shard_map(
        body,
        mesh=mesh,
        in_specs=placed,
        out_specs=(P("ep", "tp"), P("ep", "tp", None), P("ep", "tp", None), P("ep", "tp")),
        check_vma=False,
    )
```

```python
import functools

import jax
import jax.numpy as jnp
from jax import lax
from jax.experimental import pallas as pl
from jax.experimental.pallas import tpu as pltpu
from jax.sharding import PartitionSpec as P


FF2 = 16384
LANES = 128
INFO = 128
SLOTS = 2
PIECES = 8
EPS = 1e-06
SWAP = [(0, 1), (1, 0)]
F32 = jnp.float32
BF16 = jnp.bfloat16


def class_of(e):
    return (e ^ (e // 2)) % 2


def swapped(array):
    return lax.ppermute(array, "tp", SWAP)


def iota(shape, dim):
    return lax.broadcasted_iota(jnp.int32, shape, dim)


def mm(a, b):
    return jnp.dot(a, b, preferred_element_type=F32)


def mm_t(a, b):
    return lax.dot_general(a, b, (((1,), (1,)), ((), ())), preferred_element_type=F32)


def silu(v):
    return v / (1.0 + jnp.exp(-v))


def params(limit=56):
    return pltpu.CompilerParams(vmem_limit_bytes=limit << 20)


def whole(shape):
    return pl.BlockSpec(shape, lambda *_: (0,) * len(shape))


def near_call(kernel, arrays, outs, scratch=(), limit=32):
    here = pl.BlockSpec(memory_space=pltpu.VMEM)
    many = isinstance(outs, list)
    return pl.pallas_call(
        kernel,
        in_specs=[here] * len(arrays),
        out_specs=[here] * len(outs) if many else here,
        out_shape=outs,
        scratch_shapes=list(scratch),
        compiler_params=params(limit),
    )(*arrays)


def kept(ref, dim, size, other=False):
    rank = lax.axis_index("tp")
    rank = 1 - rank if other else rank
    at = pl.ds(pl.multiple_of(rank * size, size), size)
    return ref[at, :] if dim == 0 else ref[:, at]


def laid_out(ref):
    rows = ref[...].astype(F32)
    return jnp.concatenate([rows[r : r + 1, :] for r in range(rows.shape[0])], axis=1)


def tiled(vector):
    return vector.reshape(-1, LANES)


def attend_kernel(
    len_ref, fb, qg, kg, tok_f, ng_f, qw_f, kw_f, vw_f, fw_f, key_f, val_f, gate_f, ow_f,
    partial, fk_out, fv_out, cur_out,
    tok, ng, qw, kw, vw, fw, key, val, gate, ow, sems, *, block,
):
    count = tok.shape[0]
    heads = gate.shape[1]
    hd = key.shape[2]
    span = key.shape[3]
    rows = count * heads
    width = heads * hd
    scale = hd ** (-0.5)
    second = lax.axis_index("tp") == 1
    moves = []

    def fetch(far, buf):
        moves.append(pltpu.make_async_copy(far, buf, sems.at[len(moves)]))
        moves[-1].start()
        return moves[-1]

    first = [fetch(f, v) for f, v in ((tok_f, tok), (ng_f, ng))]
    loads = [fetch(f, v) for f, v in ((qw_f, qw), (kw_f, kw), (vw_f, vw), (fw_f, fw))]
    pieces = [pl.ds(at, block) for at in range(0, count, block)]
    key_moves = [fetch(key_f.at[at], key.at[at]) for at in pieces]
    gate_move = fetch(gate_f, gate)
    val_moves = [fetch(val_f.at[at], val.at[at]) for at in pieces]
    out_load = fetch(ow_f, ow)

    for move in first:
        move.wait()
    x = tok[...].astype(F32)
    ms = jnp.mean(x * x, axis=1, keepdims=True)
    normed = (x * lax.rsqrt(ms + EPS) * laid_out(ng)).astype(BF16)
    for move in loads:
        move.wait()
    q = mm(normed, qw[...])
    k = mm(normed, kw[...])
    v = mm(normed, vw[...])
    k = jnp.where(second, k[:, hd:], k[:, :hd])
    v = jnp.where(second, v[:, hd:], v[:, :hd]).astype(BF16)
    k = k * lax.rsqrt(jnp.mean(k * k, axis=1, keepdims=True) + EPS) * kg[...].astype(F32)
    k = k.astype(BF16)
    fk_out[...] = k
    fv_out[...] = v
    spread = jnp.broadcast_to(q[:, None, :], (count, heads, width)).reshape(rows, width)
    mine = iota((rows, width), 1) // hd == iota((rows, width), 0) % heads
    spread = jnp.where(mine, spread, 0.0)
    msq = jnp.sum(spread * spread, axis=1, keepdims=True) / hd
    spread = spread * lax.rsqrt(msq + EPS)
    gain = jnp.concatenate([qg[...].astype(F32)] * heads, axis=1)
    spread = (spread * gain).astype(BF16)
    pick = (iota((width, hd), 0) % hd == iota((width, hd), 1)).astype(BF16)
    queries_f = mm(spread, pick)
    queries = queries_f.astype(BF16)
    k_rows = jnp.broadcast_to(k.astype(F32)[:, None, :], (count, heads, hd)).reshape(rows, hd)
    own_all = jnp.sum(queries_f * k_rows, axis=1, keepdims=True) * scale
    v_rows = jnp.broadcast_to(v.astype(F32)[:, None, :], (count, heads, hd)).reshape(rows, hd)
    local = jnp.where(second, fw[heads:, :].astype(F32), fw[:heads, :].astype(F32)).astype(BF16)
    bias = jnp.where(second, fb[:, heads:], fb[:, :heads])
    lf = jax.nn.log_sigmoid(mm_t(normed, local) + bias)
    lf = jnp.broadcast_to(lf[:, None, :], (count, heads, heads)).reshape(rows, heads)
    lf = jnp.where(iota((rows, heads), 1) == iota((rows, heads), 0) % heads, lf, 0.0)
    lf_all = jnp.sum(lf, axis=1, keepdims=True)

    pos = iota((rows, span), 1)
    spot = iota((rows, heads), 1) == iota((rows, heads), 0) % heads
    length = jnp.concatenate(
        [jnp.full((heads, 1), len_ref[i], jnp.int32) for i in range(count)], axis=0
    )
    scores = []
    for i in range(count):
        if i % block == 0:
            key_moves[i // block].wait()
        scores.append(mm(queries[i * heads : (i + 1) * heads], key[i, 0]))
    scores = jnp.concatenate(scores, axis=0)
    gate_move.wait()
    gates = gate[...].reshape(rows, span)
    previous = jnp.sum(jnp.where(pos == length - 1, gates, 0.0), axis=1, keepdims=True)
    current = previous + lf_all
    logits = jnp.where(pos < length, scores * scale + (current - gates), -jnp.inf)
    top = jnp.maximum(jnp.max(logits, axis=1, keepdims=True), own_all)
    weights = jnp.exp(logits - top)
    own_weight = jnp.exp(own_all - top)
    total = jnp.sum(weights, axis=1, keepdims=True) + own_weight
    probs = (weights / total).astype(BF16)
    own_prob = (own_weight / total).astype(BF16).astype(F32)
    mixed = []
    for i in range(count):
        if i % block == 0:
            val_moves[i // block].wait()
        mixed.append(mm_t(probs[i * heads : (i + 1) * heads], val[i, 0]))
    mixed = jnp.concatenate(mixed, axis=0) + own_prob * v_rows
    cur = jnp.where(spot, current, 0.0).reshape(count, heads, heads)
    cur_out[...] = jnp.sum(cur, axis=1)

    pick = (iota((hd, width), 1) % hd == iota((hd, width), 0)).astype(BF16)
    wide = mm(mixed.astype(BF16), pick)
    wide = jnp.where(mine, wide, 0.0).reshape(count, heads, width)
    flat = jnp.sum(wide, axis=1).astype(BF16)
    out_load.wait()
    partial[...] = mm(flat, ow[...]).astype(BF16)


def attend(lens, tok, ng, qw, kw, vw, fw, fb, qg, kg, key, val, gate, ow):
    count, heads, _ = gate.shape
    hd = key.shape[2]
    width = tok.shape[1]
    block = 8
    big = (tok, ng, qw, kw, vw, fw, key, val, gate, ow)
    far = pl.BlockSpec(memory_space=pltpu.HBM)
    return pl.pallas_call(
        functools.partial(attend_kernel, block=block),
        grid_spec=pltpu.PrefetchScalarGridSpec(
            num_scalar_prefetch=1,
            grid=(1,),
            in_specs=[whole(fb.shape), whole(qg.shape), whole(kg.shape)] + [far] * len(big),
            out_specs=[
                whole((count, width)), whole((count, hd)), whole((count, hd)), whole((count, heads)),
            ],
            scratch_shapes=[pltpu.VMEM(a.shape, a.dtype) for a in big]
            + [
                pltpu.SemaphoreType.DMA((8 + 2 * (count // block),)),
            ],
        ),
        out_shape=[
            jax.ShapeDtypeStruct((count, width), BF16), jax.ShapeDtypeStruct((count, hd), BF16),
            jax.ShapeDtypeStruct((count, hd), BF16), jax.ShapeDtypeStruct((count, heads), F32),
        ],
        compiler_params=params(60),
        name="attend",
    )(lens, fb, qg, kg, *big)


def column(row, size):
    wide = jnp.broadcast_to(row, (size, size))
    return jnp.sum(jnp.where(iota((size, size), 0) == iota((size, size), 1), wide, 0), axis=1, keepdims=True)


def route_kernel(choice, info_out):
    count = choice.shape[1]
    picks = choice[...].astype(F32)
    earlier = iota((count, count), 1) < iota((count, count), 0)
    lane = iota((count, INFO), 1)
    info = jnp.zeros((count, INFO), F32)
    for k in range(SLOTS):
        mine_k = column(picks[k : k + 1, :], count)
        before = jnp.zeros((count, 1), F32)
        for other in range(SLOTS):
            same = jnp.logical_and(mine_k == picks[other : other + 1, :], earlier)
            before += jnp.sum(jnp.where(same, 1.0, 0.0), axis=1, keepdims=True)
        info = jnp.where(lane == k, mine_k * SLOTS + before, info)
    info_out[...] = info


def route(choice):
    out = jax.ShapeDtypeStruct((choice.shape[1], INFO), F32)
    return near_call(route_kernel, (choice,), out, limit=4)


def norm_kernel(tok, mine, theirs, pg, bg, info, copies, resid_out, branch_out):
    count, width = tok.shape
    half = width // 2
    second = lax.axis_index("tp") == 1
    attn = mine[...].astype(F32) + theirs[...].astype(F32)
    resid = (tok[...].astype(F32) + attn).astype(BF16).astype(F32)
    ms = jnp.mean(resid * resid, axis=1, keepdims=True)
    post = (resid * lax.rsqrt(ms + EPS) * laid_out(pg)).astype(BF16).astype(F32)
    line = jnp.concatenate(
        [jnp.where(second, post[:, half:], post[:, :half]), info[...]], axis=1
    ).astype(BF16)
    for peer in range(copies.shape[0]):
        copies[peer] = line
    logit = jnp.sum(post * laid_out(bg), axis=1, keepdims=True)
    branch_out[...] = jnp.broadcast_to(1.0 / (1.0 + jnp.exp(-logit)), (count, LANES))
    resid_out[...] = jnp.where(second, resid[:, half:], resid[:, :half]).astype(BF16)


def normalize(tok, mine, theirs, pg, bg, info, peers):
    count, width = tok.shape
    half = width // 2
    outs = [
        jax.ShapeDtypeStruct((peers, count, half + INFO), BF16),
        jax.ShapeDtypeStruct((count, half), BF16),
        jax.ShapeDtypeStruct((count, LANES), F32),
    ]
    return near_call(norm_kernel, (tok, mine, theirs, pg, bg, info), outs, limit=8)


def pack_kernel(*refs):
    weights, (out, sems) = refs[:-2], refs[-2:]
    half = out.shape[0]
    units = weights[0].shape[1]
    at = pl.ds(pl.multiple_of(lax.axis_index("tp") * half, half), half)
    moves = [
        pltpu.make_async_copy(w.at[at, :], out.at[:, pl.ds(n * units, units)], sems.at[n])
        for n, w in enumerate(weights)
    ]
    for move in moves:
        move.start()
    for move in moves:
        move.wait()


def pack_down_kernel(*refs):
    weights, (out, sems) = refs[:-2], refs[-2:]
    half = out.shape[1]
    units = weights[0].shape[0]
    at = pl.ds(pl.multiple_of(lax.axis_index("tp") * half, half), half)
    moves = [
        pltpu.make_async_copy(w.at[:, at], out.at[pl.ds(n * units, units), :], sems.at[n])
        for n, w in enumerate(weights)
    ]
    for move in moves:
        move.start()
    for move in moves:
        move.wait()


def pack(kernel, weights, shape):
    return pl.pallas_call(
        kernel,
        in_specs=[pl.BlockSpec(memory_space=pltpu.HBM)] * len(weights),
        out_specs=pl.BlockSpec(memory_space=pltpu.VMEM),
        out_shape=jax.ShapeDtypeStruct(shape, BF16),
        scratch_shapes=[pltpu.SemaphoreType.DMA((len(weights),))],
        compiler_params=params(16),
    )(*weights)


def hidden_kernel(x, wide, out):
    half = wide.shape[0]
    tokens = x[:, :half]
    for b in range(wide.shape[1] // 256):
        at = slice(256 * b, 256 * (b + 1))
        out[:, at] = mm(tokens, wide[:, at]).astype(BF16)


def dense_hidden(lines, wide):
    out = jax.ShapeDtypeStruct((lines.shape[0], wide.shape[1]), BF16)
    return near_call(hidden_kernel, (lines, wide), out, limit=16)


def extract_kernel(x, own_rows, near_rows, *, count):
    total = x.shape[0]
    half = own_rows.shape[1]
    peers = total // count
    shape = (total, 4 * peers)
    col = iota((1, 4 * peers), 1)
    expert = lax.axis_index("ep") ^ (col // (2 * peers))
    want = (expert * SLOTS + (col // peers) % 2).astype(F32)
    low = (col % peers) * count
    token = iota(shape, 0)
    info = x[:, half:].astype(F32)
    hit = jnp.logical_or(info[:, 0:1] == want, info[:, 1:2] == want)
    hit = jnp.logical_and(hit, jnp.logical_and(token >= low, token < low + count))
    pick = jnp.where(hit, 1.0, 0.0).astype(BF16)
    rows = lax.dot_general(
        pick, x[:, :half], (((0,), (0,)), ((), ())), preferred_element_type=F32
    ).astype(BF16)
    own_rows[...] = rows[: 2 * peers, :]
    near_rows[...] = rows[2 * peers :, :]


def extract(lines, count):
    total, wide = lines.shape
    rows = jax.ShapeDtypeStruct((2 * total // count, wide - INFO), BF16)
    kernel = functools.partial(extract_kernel, count=count)
    return near_call(kernel, (lines,), [rows, rows], limit=16)


def down_kernel(mine, theirs, down, far, squares_far, out, hid, squares, sems, *, count, block):
    units = mine.shape[1] // 8
    total, _ = out.shape
    peers = total // count
    steps = [slice(at, at + block) for at in range(0, total, block)]
    part = jnp.zeros((peers, LANES), F32)
    for at in steps:

        def full(b):
            there = b ^ 1
            return mine[at, b * units : (b + 1) * units].astype(F32) + theirs[
                at, there * units : (there + 1) * units
            ].astype(F32)

        hidden = [silu(full(b)) * full(b + 2) for b in (0, 1, 4, 5)]
        square = jnp.sum(sum(h * h for h in hidden), axis=1, keepdims=True)
        hid[at, :] = jnp.concatenate([a.astype(BF16) for a in hidden], axis=1)
        token = iota((block, LANES), 0) + at.start
        spread = jnp.where(iota((block, LANES), 1) == token % count, square, 0.0)
        high = spread.astype(BF16)
        low = (spread - high.astype(F32)).astype(BF16)
        here = iota((peers, block), 1) + at.start
        start = iota((peers, block), 0) * count
        owner = jnp.logical_and(here >= start, here < start + count)
        owner = jnp.where(owner, 1.0, 0.0).astype(BF16)
        part += mm(owner, high) + mm(owner, low)
    squares[...] = part
    moves = [pltpu.make_async_copy(squares, squares_far, sems.at[0])]
    moves[0].start()
    for n, at in enumerate(steps):
        out[at, :] = mm(hid[at, :], down[...]).astype(BF16)
        moves.append(pltpu.make_async_copy(out.at[at, :], far.at[at, :], sems.at[n + 1]))
        moves[-1].start()
    for move in moves:
        move.wait()


def dense_down(mine, theirs, down, count):
    total = mine.shape[0]
    units, half = down.shape
    block = 256
    here = pl.BlockSpec(memory_space=pltpu.VMEM)
    far = pl.BlockSpec(memory_space=pltpu.HBM)
    return pl.pallas_call(
        functools.partial(down_kernel, count=count, block=block),
        in_specs=[here] * 3,
        out_specs=[far, far],
        out_shape=[
            jax.ShapeDtypeStruct((total, half), BF16),
            jax.ShapeDtypeStruct((total // count, LANES), F32),
        ],
        scratch_shapes=[
            pltpu.VMEM((total, half), BF16), pltpu.VMEM((total, units), BF16),
            pltpu.VMEM((total // count, LANES), F32),
            pltpu.SemaphoreType.DMA((total // block + 1,)),
        ],
        compiler_params=params(16),
        name="dense_down",
    )(mine, theirs, down)


def expert_kernel(a0, b0, a1, b1, gw, uw, dw, after, keep, give, gbuf, ubuf, dbuf, sems):
    half = a0.shape[1]
    moves = []
    for n, (far, buf) in enumerate(((gw, gbuf), (uw, ubuf), (dw, dbuf))):
        part = buf.shape[0] // PIECES
        for m in range(PIECES):
            at = pl.ds(m * part, part)
            moves.append(
                pltpu.make_async_copy(far.at[0, at, :], buf.at[at, :], sems.at[PIECES * n + m])
            )
            moves[-1].start()
    x0 = jnp.concatenate([a0[...], b0[...]], axis=0)
    x1 = jnp.concatenate([a1[...], b1[...]], axis=0)

    def rows(w):
        return mm(x0, kept(w, 0, half)) + mm(x1, kept(w, 0, half, True))

    for move in moves[:PIECES]:
        move.wait()
    gate = silu(rows(gbuf))
    for move in moves[PIECES : 2 * PIECES]:
        move.wait()
    act = (gate * rows(ubuf)).astype(BF16)
    for move in moves[2 * PIECES :]:
        move.wait()
    keep[...] = mm(act, kept(dbuf, 1, half)).astype(BF16)
    give[...] = mm(act, kept(dbuf, 1, half, True)).astype(BF16)


def experts(rows, away, gate_w, up_w, down_w, after):
    count, half = rows[0].shape
    here = pl.BlockSpec(memory_space=pltpu.VMEM)
    far = pl.BlockSpec(memory_space=pltpu.HBM)
    return pl.pallas_call(
        expert_kernel,
        in_specs=[here] * 4 + [far] * 3 + [here],
        out_specs=[here] * 2,
        out_shape=[jax.ShapeDtypeStruct((2 * count, half), BF16)] * 2,
        scratch_shapes=[pltpu.VMEM(w.shape[1:], BF16) for w in (gate_w, up_w, down_w)]
        + [pltpu.SemaphoreType.DMA((3 * PIECES,))],
        compiler_params=params(52),
        name="experts",
    )(*rows, *away, gate_w, up_w, down_w, after)


def merge_kernel(keep, other, near):
    half = near.shape[0]
    near[...] = (keep[half:, :].astype(F32) + other[half:, :].astype(F32)).astype(BF16)


def merge(keep, other):
    out = jax.ShapeDtypeStruct((keep.shape[0] // 2, keep.shape[1]), BF16)
    return near_call(merge_kernel, (keep, other), out, limit=16)


def answer_kernel(keep, other, near, squares, out, scr):
    peers = out.shape[0]
    half = near.shape[0]
    own = keep[:half, :].astype(F32) + other[:half, :].astype(F32)
    parts = own.shape[1] // LANES
    for g, total in enumerate((own, near[...].astype(F32))):
        for s in range(SLOTS):
            for f in range(parts):
                scr[:, parts * (SLOTS * g + s) + f, :] = total[
                    peers * s : peers * (s + 1), LANES * f : LANES * (f + 1)
                ]
    out[:, : 2 * SLOTS * parts, :] = scr[...].astype(BF16)
    out[:, 2 * SLOTS * parts :, :] = jnp.broadcast_to(
        squares[...][:, None, :], (peers, 8, LANES)
    ).astype(BF16)


def answers(keep, other, near, squares):
    peers = squares.shape[0]
    rows = 2 * SLOTS * keep.shape[1] // LANES
    out = jax.ShapeDtypeStruct((peers, rows + 8, LANES), BF16)
    scratch = [pltpu.VMEM((peers, rows, LANES), F32)]
    return near_call(answer_kernel, (keep, other, near, squares), out, scratch, limit=16)


def last_kernel(returned, parts, info, weight, branch, resid, out, scr):
    count, half = resid.shape
    peers = returned.shape[0]
    tiles = half // LANES
    rows = 2 * SLOTS * tiles
    scr[...] = returned[:, :rows, :].astype(F32)
    values = jnp.concatenate(
        [
            jnp.concatenate([scr[:, tiles * b + f, :] for f in range(tiles)], axis=1)
            for b in range(2 * SLOTS)
        ],
        axis=0,
    ).astype(BF16)
    lane = iota((1, 2 * SLOTS * peers), 1)
    peer = lane % peers
    expert = (2 * peer + (peer + class_of(lax.axis_index("ep"))) % 2) ^ (lane // (SLOTS * peers))
    code = (expert * SLOTS + (lane // peers) % SLOTS).astype(F32)
    expert_sum = jnp.zeros((count, half), F32)
    for k in range(SLOTS):
        pick = jnp.where(info[:, k : k + 1] == code, 1.0, 0.0).astype(BF16)
        expert_sum += column(weight[k : k + 1, :], count) * mm(pick, values)
    square = jnp.sum(returned[:, rows : rows + 8, :].astype(F32), axis=0)
    square = column(square[0:1, :count], count)
    dense = jnp.sum(parts[...].astype(F32), axis=0)
    dense = (dense * lax.rsqrt(square / FF2 + EPS)).astype(BF16).astype(F32)
    out[...] = (resid[...].astype(F32) + expert_sum + branch[:, :1] * dense).astype(BF16)


def last_sum(returned, parts, info, weight, branch, resid):
    arrays = (returned, parts, info, weight, branch, resid)
    out = jax.ShapeDtypeStruct(resid.shape, BF16)
    scratch = [pltpu.VMEM((returned.shape[0], 2 * SLOTS * resid.shape[1] // LANES, LANES), F32)]
    return near_call(last_kernel, arrays, out, scratch, limit=16)


def body(
    tokens,
    norm_gain,
    query_w,
    key_w,
    value_w,
    forget_w,
    forget_bias,
    query_gain,
    key_gain,
    cache_key,
    cache_value,
    cache_gate,
    cache_len,
    out_w,
    post_gain,
    branch_gate,
    dense_gate_w,
    dense_up_w,
    dense_down_w,
    expert_choice,
    route_weight,
    expert_gate_w,
    expert_up_w,
    expert_down_w,
):
    count = tokens.shape[0]
    ep_count = lax.axis_size("ep")
    peers = ep_count // 2
    pair = [(e, e ^ 1) for e in range(ep_count)]
    classes = [[e for e in range(ep_count) if class_of(e) == c] for c in range(2)]

    near = []
    for array in (dense_gate_w, dense_up_w, dense_down_w):
        near.append(lax.ppermute(array, "ep", pair))

    partial, fresh_key, fresh_value, current = attend(
        cache_len, tokens, tiled(norm_gain), query_w, key_w, value_w, forget_w.T,
        forget_bias[None], query_gain[None], key_gain[None], cache_key, cache_value,
        cache_gate, out_w,
    )
    partial_other = swapped(partial)
    info = route(expert_choice.T)
    copies, resid, branch = normalize(
        tokens, partial, partial_other, tiled(post_gain), tiled(branch_gate), info, peers
    )
    lines = lax.all_to_all(copies, "ep", 0, 0, tiled=True, axis_index_groups=classes)
    lines = lines.reshape(peers * count, -1)

    gate_up = []
    for array in (dense_gate_w, dense_up_w, near[0], near[1]):
        gate_up += [array, swapped(array)]
    downs = []
    for down_w in (dense_down_w, near[2]):
        downs += [down_w, swapped(down_w)]

    width, units = dense_gate_w.shape
    wide = pack(pack_kernel, gate_up, (width // 2, len(gate_up) * units))
    down = pack(pack_down_kernel, downs, (len(downs) * units, width // 2))
    part = dense_hidden(lines, wide)
    part_other = swapped(part)
    own_rows, near_rows = extract(lines, count)
    pair_rows = lax.ppermute(near_rows, "ep", pair)
    terms, squares = dense_down(part, part_other, down, count)
    parts = lax.all_to_all(
        terms.reshape(peers, count, -1), "ep", 0, 0, tiled=True, axis_index_groups=classes
    )

    away = (swapped(own_rows), swapped(pair_rows))
    keep, give = experts(
        (own_rows, pair_rows), away, expert_gate_w, expert_up_w, expert_down_w, squares
    )
    other = swapped(give)
    back = lax.ppermute(merge(keep, other), "ep", pair)
    answer = answers(keep, other, back, squares)
    returned = lax.all_to_all(answer, "ep", 0, 0, tiled=True, axis_index_groups=classes)
    mixed_out = last_sum(returned, parts, info, route_weight.T, branch, resid)
    return (mixed_out, fresh_key[:, None, :], fresh_value[:, None, :], current)


def solution(mesh):
    placed = (
        P("ep", None),
        P(),
        P(None, "tp"),
        P(),
        P(),
        P(),
        P(),
        P(),
        P(),
        P("ep", "tp", None, None),
        P("ep", "tp", None, None),
        P("ep", "tp", None),
        P("ep"),
        P("tp", None),
        P(),
        P(),
        P(None, ("ep", "tp")),
        P(None, ("ep", "tp")),
        P(("ep", "tp"), None),
        P("ep", None),
        P("ep", None),
        P("ep", None, "tp"),
        P("ep", None, "tp"),
        P("ep", "tp", None),
    )

    return jax.shard_map(
        body,
        mesh=mesh,
        in_specs=placed,
        out_specs=(P("ep", "tp"), P("ep", "tp", None), P("ep", "tp", None), P("ep", "tp")),
        check_vma=False,
    )
```

```python
import functools

import jax
import jax.numpy as jnp
from jax import lax
from jax.experimental import pallas as pl
from jax.experimental.pallas import tpu as pltpu
from jax.sharding import PartitionSpec as P


FF2 = 16384
LANES = 128
INFO = 128
SLOTS = 2
PIECES = 8
EPS = 1e-06
SWAP = [(0, 1), (1, 0)]
F32 = jnp.float32
BF16 = jnp.bfloat16


def class_of(e):
    return (e ^ (e // 2)) % 2


def swapped(array):
    return lax.ppermute(array, "tp", SWAP)


def iota(shape, dim):
    return lax.broadcasted_iota(jnp.int32, shape, dim)


def mm(a, b):
    return jnp.dot(a, b, preferred_element_type=F32)


def mm_t(a, b):
    return lax.dot_general(a, b, (((1,), (1,)), ((), ())), preferred_element_type=F32)


def silu(v):
    return v / (1.0 + jnp.exp(-v))


def params(limit=56):
    return pltpu.CompilerParams(vmem_limit_bytes=limit << 20)


def whole(shape):
    return pl.BlockSpec(shape, lambda *_: (0,) * len(shape))


def near_call(kernel, arrays, outs, scratch=(), limit=32):
    here = pl.BlockSpec(memory_space=pltpu.VMEM)
    many = isinstance(outs, list)
    return pl.pallas_call(
        kernel,
        in_specs=[here] * len(arrays),
        out_specs=[here] * len(outs) if many else here,
        out_shape=outs,
        scratch_shapes=list(scratch),
        compiler_params=params(limit),
    )(*arrays)


def kept(ref, dim, size, other=False):
    rank = lax.axis_index("tp")
    rank = 1 - rank if other else rank
    at = pl.ds(pl.multiple_of(rank * size, size), size)
    return ref[at, :] if dim == 0 else ref[:, at]


def laid_out(ref):
    rows = ref[...].astype(F32)
    return jnp.concatenate([rows[r : r + 1, :] for r in range(rows.shape[0])], axis=1)


def tiled(vector):
    return vector.reshape(-1, LANES)


def attend_kernel(
    len_ref, fb, qg, kg, tok_f, ng_f, qw_f, kw_f, vw_f, fw_f, key_f, val_f, gate_f, ow_f,
    partial, fk_out, fv_out, cur_out,
    tok, ng, qw, kw, vw, fw, key, val, gate, ow, sems, *, block,
):
    count = tok.shape[0]
    heads = gate.shape[1]
    hd = key.shape[2]
    span = key.shape[3]
    rows = count * heads
    width = heads * hd
    scale = hd ** (-0.5)
    second = lax.axis_index("tp") == 1
    moves = []

    def fetch(far, buf):
        moves.append(pltpu.make_async_copy(far, buf, sems.at[len(moves)]))
        moves[-1].start()
        return moves[-1]

    first = [fetch(f, v) for f, v in ((tok_f, tok), (ng_f, ng))]
    loads = [fetch(f, v) for f, v in ((qw_f, qw), (kw_f, kw), (vw_f, vw), (fw_f, fw))]
    pieces = [pl.ds(at, block) for at in range(0, count, block)]
    key_moves = [fetch(key_f.at[at], key.at[at]) for at in pieces]
    gate_move = fetch(gate_f, gate)
    val_moves = [fetch(val_f.at[at], val.at[at]) for at in pieces]
    out_load = fetch(ow_f, ow)

    for move in first:
        move.wait()
    x = tok[...].astype(F32)
    ms = jnp.mean(x * x, axis=1, keepdims=True)
    normed = (x * lax.rsqrt(ms + EPS) * laid_out(ng)).astype(BF16)
    for move in loads:
        move.wait()
    q = mm(normed, qw[...])
    k = mm(normed, kw[...])
    v = mm(normed, vw[...])
    k = jnp.where(second, k[:, hd:], k[:, :hd])
    v = jnp.where(second, v[:, hd:], v[:, :hd]).astype(BF16)
    k = k * lax.rsqrt(jnp.mean(k * k, axis=1, keepdims=True) + EPS) * kg[...].astype(F32)
    k = k.astype(BF16)
    fk_out[...] = k
    fv_out[...] = v
    spread = jnp.broadcast_to(q[:, None, :], (count, heads, width)).reshape(rows, width)
    mine = iota((rows, width), 1) // hd == iota((rows, width), 0) % heads
    spread = jnp.where(mine, spread, 0.0)
    msq = jnp.sum(spread * spread, axis=1, keepdims=True) / hd
    spread = spread * lax.rsqrt(msq + EPS)
    gain = jnp.concatenate([qg[...].astype(F32)] * heads, axis=1)
    spread = (spread * gain).astype(BF16)
    pick = (iota((width, hd), 0) % hd == iota((width, hd), 1)).astype(BF16)
    queries_f = mm(spread, pick)
    queries = queries_f.astype(BF16)
    k_rows = jnp.broadcast_to(k.astype(F32)[:, None, :], (count, heads, hd)).reshape(rows, hd)
    own_all = jnp.sum(queries_f * k_rows, axis=1, keepdims=True) * scale
    v_rows = jnp.broadcast_to(v.astype(F32)[:, None, :], (count, heads, hd)).reshape(rows, hd)
    local = jnp.where(second, fw[heads:, :].astype(F32), fw[:heads, :].astype(F32)).astype(BF16)
    bias = jnp.where(second, fb[:, heads:], fb[:, :heads])
    lf = jax.nn.log_sigmoid(mm_t(normed, local) + bias)
    lf = jnp.broadcast_to(lf[:, None, :], (count, heads, heads)).reshape(rows, heads)
    lf = jnp.where(iota((rows, heads), 1) == iota((rows, heads), 0) % heads, lf, 0.0)
    lf_all = jnp.sum(lf, axis=1, keepdims=True)

    pos = iota((rows, span), 1)
    spot = iota((rows, heads), 1) == iota((rows, heads), 0) % heads
    length = jnp.concatenate(
        [jnp.full((heads, 1), len_ref[i], jnp.int32) for i in range(count)], axis=0
    )
    scores = []
    for i in range(count):
        if i % block == 0:
            key_moves[i // block].wait()
        scores.append(mm(queries[i * heads : (i + 1) * heads], key[i, 0]))
    scores = jnp.concatenate(scores, axis=0)
    gate_move.wait()
    gates = gate[...].reshape(rows, span)
    previous = jnp.sum(jnp.where(pos == length - 1, gates, 0.0), axis=1, keepdims=True)
    current = previous + lf_all
    logits = jnp.where(pos < length, scores * scale + (current - gates), -jnp.inf)
    top = jnp.maximum(jnp.max(logits, axis=1, keepdims=True), own_all)
    weights = jnp.exp(logits - top)
    own_weight = jnp.exp(own_all - top)
    total = jnp.sum(weights, axis=1, keepdims=True) + own_weight
    probs = (weights / total).astype(BF16)
    own_prob = (own_weight / total).astype(BF16).astype(F32)
    mixed = []
    for i in range(count):
        if i % block == 0:
            val_moves[i // block].wait()
        mixed.append(mm_t(probs[i * heads : (i + 1) * heads], val[i, 0]))
    mixed = jnp.concatenate(mixed, axis=0) + own_prob * v_rows
    cur = jnp.where(spot, current, 0.0).reshape(count, heads, heads)
    cur_out[...] = jnp.sum(cur, axis=1)

    pick = (iota((hd, width), 1) % hd == iota((hd, width), 0)).astype(BF16)
    wide = mm(mixed.astype(BF16), pick)
    wide = jnp.where(mine, wide, 0.0).reshape(count, heads, width)
    flat = jnp.sum(wide, axis=1).astype(BF16)
    out_load.wait()
    partial[...] = mm(flat, ow[...]).astype(BF16)


def attend(lens, tok, ng, qw, kw, vw, fw, fb, qg, kg, key, val, gate, ow):
    count, heads, _ = gate.shape
    hd = key.shape[2]
    width = tok.shape[1]
    block = 8
    big = (tok, ng, qw, kw, vw, fw, key, val, gate, ow)
    far = pl.BlockSpec(memory_space=pltpu.HBM)
    return pl.pallas_call(
        functools.partial(attend_kernel, block=block),
        grid_spec=pltpu.PrefetchScalarGridSpec(
            num_scalar_prefetch=1,
            grid=(1,),
            in_specs=[whole(fb.shape), whole(qg.shape), whole(kg.shape)] + [far] * len(big),
            out_specs=[
                whole((count, width)), whole((count, hd)), whole((count, hd)), whole((count, heads)),
            ],
            scratch_shapes=[pltpu.VMEM(a.shape, a.dtype) for a in big]
            + [
                pltpu.SemaphoreType.DMA((8 + 2 * (count // block),)),
            ],
        ),
        out_shape=[
            jax.ShapeDtypeStruct((count, width), BF16), jax.ShapeDtypeStruct((count, hd), BF16),
            jax.ShapeDtypeStruct((count, hd), BF16), jax.ShapeDtypeStruct((count, heads), F32),
        ],
        compiler_params=params(60),
        name="attend",
    )(lens, fb, qg, kg, *big)


def column(row, size):
    wide = jnp.broadcast_to(row, (size, size))
    return jnp.sum(jnp.where(iota((size, size), 0) == iota((size, size), 1), wide, 0), axis=1, keepdims=True)


def route_kernel(choice, info_out):
    count = choice.shape[1]
    picks = choice[...].astype(F32)
    earlier = iota((count, count), 1) < iota((count, count), 0)
    lane = iota((count, INFO), 1)
    info = jnp.zeros((count, INFO), F32)
    for k in range(SLOTS):
        mine_k = column(picks[k : k + 1, :], count)
        before = jnp.zeros((count, 1), F32)
        for other in range(SLOTS):
            same = jnp.logical_and(mine_k == picks[other : other + 1, :], earlier)
            before += jnp.sum(jnp.where(same, 1.0, 0.0), axis=1, keepdims=True)
        info = jnp.where(lane == k, mine_k * SLOTS + before, info)
    info_out[...] = info


def route(choice):
    out = jax.ShapeDtypeStruct((choice.shape[1], INFO), F32)
    return near_call(route_kernel, (choice,), out, limit=4)


def norm_kernel(tok, mine, theirs, pg, bg, info, copies, resid_out, branch_out):
    count, width = tok.shape
    half = width // 2
    second = lax.axis_index("tp") == 1
    attn = mine[...].astype(F32) + theirs[...].astype(F32)
    resid = (tok[...].astype(F32) + attn).astype(BF16).astype(F32)
    ms = jnp.mean(resid * resid, axis=1, keepdims=True)
    post = (resid * lax.rsqrt(ms + EPS) * laid_out(pg)).astype(BF16).astype(F32)
    line = jnp.concatenate(
        [jnp.where(second, post[:, half:], post[:, :half]), info[...]], axis=1
    ).astype(BF16)
    for peer in range(copies.shape[0]):
        copies[peer] = line
    logit = jnp.sum(post * laid_out(bg), axis=1, keepdims=True)
    branch_out[...] = jnp.broadcast_to(1.0 / (1.0 + jnp.exp(-logit)), (count, LANES))
    resid_out[...] = jnp.where(second, resid[:, half:], resid[:, :half]).astype(BF16)


def normalize(tok, mine, theirs, pg, bg, info, peers):
    count, width = tok.shape
    half = width // 2
    outs = [
        jax.ShapeDtypeStruct((peers, count, half + INFO), BF16),
        jax.ShapeDtypeStruct((count, half), BF16),
        jax.ShapeDtypeStruct((count, LANES), F32),
    ]
    return near_call(norm_kernel, (tok, mine, theirs, pg, bg, info), outs, limit=8)


def pack_kernel(*refs):
    weights, (out, sems) = refs[:-2], refs[-2:]
    half = out.shape[0]
    units = weights[0].shape[1]
    at = pl.ds(pl.multiple_of(lax.axis_index("tp") * half, half), half)
    moves = [
        pltpu.make_async_copy(w.at[at, :], out.at[:, pl.ds(n * units, units)], sems.at[n])
        for n, w in enumerate(weights)
    ]
    for move in moves:
        move.start()
    for move in moves:
        move.wait()


def pack_down_kernel(*refs):
    weights, (out, sems) = refs[:-2], refs[-2:]
    half = out.shape[1]
    units = weights[0].shape[0]
    at = pl.ds(pl.multiple_of(lax.axis_index("tp") * half, half), half)
    moves = [
        pltpu.make_async_copy(w.at[:, at], out.at[pl.ds(n * units, units), :], sems.at[n])
        for n, w in enumerate(weights)
    ]
    for move in moves:
        move.start()
    for move in moves:
        move.wait()


def pack(kernel, weights, shape):
    return pl.pallas_call(
        kernel,
        in_specs=[pl.BlockSpec(memory_space=pltpu.HBM)] * len(weights),
        out_specs=pl.BlockSpec(memory_space=pltpu.VMEM),
        out_shape=jax.ShapeDtypeStruct(shape, BF16),
        scratch_shapes=[pltpu.SemaphoreType.DMA((len(weights),))],
        compiler_params=params(16),
    )(*weights)


def hidden_kernel(x, own, far, out):
    half, cols = own.shape
    tokens = x[:, :half]
    for n, wide in enumerate((own, far)):
        for b in range(0, cols, 256):
            out[:, n * cols + b : n * cols + b + 256] = mm(tokens, wide[:, b : b + 256]).astype(BF16)


def dense_hidden(lines, own, far):
    out = jax.ShapeDtypeStruct((lines.shape[0], 2 * own.shape[1]), BF16)
    return near_call(hidden_kernel, (lines, own, far), out, limit=16)


def extract_kernel(x, own_rows, near_rows, *, count):
    total = x.shape[0]
    half = own_rows.shape[1]
    peers = total // count
    shape = (total, 4 * peers)
    col = iota((1, 4 * peers), 1)
    expert = lax.axis_index("ep") ^ (col // (2 * peers))
    want = (expert * SLOTS + (col // peers) % 2).astype(F32)
    low = (col % peers) * count
    token = iota(shape, 0)
    info = x[:, half:].astype(F32)
    hit = jnp.logical_or(info[:, 0:1] == want, info[:, 1:2] == want)
    hit = jnp.logical_and(hit, jnp.logical_and(token >= low, token < low + count))
    pick = jnp.where(hit, 1.0, 0.0).astype(BF16)
    rows = lax.dot_general(
        pick, x[:, :half], (((0,), (0,)), ((), ())), preferred_element_type=F32
    ).astype(BF16)
    own_rows[...] = rows[: 2 * peers, :]
    near_rows[...] = rows[2 * peers :, :]


def extract(lines, count):
    total, wide = lines.shape
    rows = jax.ShapeDtypeStruct((2 * total // count, wide - INFO), BF16)
    kernel = functools.partial(extract_kernel, count=count)
    return near_call(kernel, (lines,), [rows, rows], limit=16)


def down_kernel(mine, theirs, down, far, squares_far, out, hid, squares, sems, *, count, block):
    units = mine.shape[1] // 8
    total, _ = out.shape
    peers = total // count
    steps = [slice(at, at + block) for at in range(0, total, block)]
    part = jnp.zeros((peers, LANES), F32)
    for at in steps:

        def full(b):
            there = b ^ 1
            return mine[at, b * units : (b + 1) * units].astype(F32) + theirs[
                at, there * units : (there + 1) * units
            ].astype(F32)

        hidden = [silu(full(b)) * full(b + 2) for b in (0, 1, 4, 5)]
        square = jnp.sum(sum(h * h for h in hidden), axis=1, keepdims=True)
        hid[at, :] = jnp.concatenate([a.astype(BF16) for a in hidden], axis=1)
        token = iota((block, LANES), 0) + at.start
        spread = jnp.where(iota((block, LANES), 1) == token % count, square, 0.0)
        high = spread.astype(BF16)
        low = (spread - high.astype(F32)).astype(BF16)
        here = iota((peers, block), 1) + at.start
        start = iota((peers, block), 0) * count
        owner = jnp.logical_and(here >= start, here < start + count)
        owner = jnp.where(owner, 1.0, 0.0).astype(BF16)
        part += mm(owner, high) + mm(owner, low)
    squares[...] = part
    moves = [pltpu.make_async_copy(squares, squares_far, sems.at[0])]
    moves[0].start()
    for n, at in enumerate(steps):
        out[at, :] = mm(hid[at, :], down[...]).astype(BF16)
        moves.append(pltpu.make_async_copy(out.at[at, :], far.at[at, :], sems.at[n + 1]))
        moves[-1].start()
    for move in moves:
        move.wait()


def dense_down(mine, theirs, down, count):
    total = mine.shape[0]
    units, half = down.shape
    block = 256
    here = pl.BlockSpec(memory_space=pltpu.VMEM)
    far = pl.BlockSpec(memory_space=pltpu.HBM)
    return pl.pallas_call(
        functools.partial(down_kernel, count=count, block=block),
        in_specs=[here] * 3,
        out_specs=[far, far],
        out_shape=[
            jax.ShapeDtypeStruct((total, half), BF16),
            jax.ShapeDtypeStruct((total // count, LANES), F32),
        ],
        scratch_shapes=[
            pltpu.VMEM((total, half), BF16), pltpu.VMEM((total, units), BF16),
            pltpu.VMEM((total // count, LANES), F32),
            pltpu.SemaphoreType.DMA((total // block + 1,)),
        ],
        compiler_params=params(16),
        name="dense_down",
    )(mine, theirs, down)


def expert_kernel(a0, b0, a1, b1, gw, uw, dw, after, keep, give, gbuf, ubuf, dbuf, sems):
    half = a0.shape[1]
    moves = []
    for n, (far, buf) in enumerate(((gw, gbuf), (uw, ubuf), (dw, dbuf))):
        part = buf.shape[0] // PIECES
        for m in range(PIECES):
            at = pl.ds(m * part, part)
            moves.append(
                pltpu.make_async_copy(far.at[0, at, :], buf.at[at, :], sems.at[PIECES * n + m])
            )
            moves[-1].start()
    x0 = jnp.concatenate([a0[...], b0[...]], axis=0)
    x1 = jnp.concatenate([a1[...], b1[...]], axis=0)

    def rows(w):
        return mm(x0, kept(w, 0, half)) + mm(x1, kept(w, 0, half, True))

    for move in moves[:PIECES]:
        move.wait()
    gate = silu(rows(gbuf))
    for move in moves[PIECES : 2 * PIECES]:
        move.wait()
    act = (gate * rows(ubuf)).astype(BF16)
    for move in moves[2 * PIECES :]:
        move.wait()
    keep[...] = mm(act, kept(dbuf, 1, half)).astype(BF16)
    give[...] = mm(act, kept(dbuf, 1, half, True)).astype(BF16)


def experts(rows, away, gate_w, up_w, down_w, after):
    count, half = rows[0].shape
    here = pl.BlockSpec(memory_space=pltpu.VMEM)
    far = pl.BlockSpec(memory_space=pltpu.HBM)
    return pl.pallas_call(
        expert_kernel,
        in_specs=[here] * 4 + [far] * 3 + [here],
        out_specs=[here] * 2,
        out_shape=[jax.ShapeDtypeStruct((2 * count, half), BF16)] * 2,
        scratch_shapes=[pltpu.VMEM(w.shape[1:], BF16) for w in (gate_w, up_w, down_w)]
        + [pltpu.SemaphoreType.DMA((3 * PIECES,))],
        compiler_params=params(52),
        name="experts",
    )(*rows, *away, gate_w, up_w, down_w, after)


def merge_kernel(keep, other, near):
    half = near.shape[0]
    near[...] = (keep[half:, :].astype(F32) + other[half:, :].astype(F32)).astype(BF16)


def merge(keep, other):
    out = jax.ShapeDtypeStruct((keep.shape[0] // 2, keep.shape[1]), BF16)
    return near_call(merge_kernel, (keep, other), out, limit=16)


def answer_kernel(keep, other, near, squares, out, scr):
    peers = out.shape[0]
    half = near.shape[0]
    own = keep[:half, :].astype(F32) + other[:half, :].astype(F32)
    parts = own.shape[1] // LANES
    for g, total in enumerate((own, near[...].astype(F32))):
        for s in range(SLOTS):
            for f in range(parts):
                scr[:, parts * (SLOTS * g + s) + f, :] = total[
                    peers * s : peers * (s + 1), LANES * f : LANES * (f + 1)
                ]
    out[:, : 2 * SLOTS * parts, :] = scr[...].astype(BF16)
    out[:, 2 * SLOTS * parts :, :] = jnp.broadcast_to(
        squares[...][:, None, :], (peers, 8, LANES)
    ).astype(BF16)


def answers(keep, other, near, squares):
    peers = squares.shape[0]
    rows = 2 * SLOTS * keep.shape[1] // LANES
    out = jax.ShapeDtypeStruct((peers, rows + 8, LANES), BF16)
    scratch = [pltpu.VMEM((peers, rows, LANES), F32)]
    return near_call(answer_kernel, (keep, other, near, squares), out, scratch, limit=16)


def last_kernel(returned, parts, info, weight, branch, resid, out, scr):
    count, half = resid.shape
    peers = returned.shape[0]
    tiles = half // LANES
    rows = 2 * SLOTS * tiles
    scr[...] = returned[:, :rows, :].astype(F32)
    values = jnp.concatenate(
        [
            jnp.concatenate([scr[:, tiles * b + f, :] for f in range(tiles)], axis=1)
            for b in range(2 * SLOTS)
        ],
        axis=0,
    ).astype(BF16)
    lane = iota((1, 2 * SLOTS * peers), 1)
    peer = lane % peers
    expert = (2 * peer + (peer + class_of(lax.axis_index("ep"))) % 2) ^ (lane // (SLOTS * peers))
    code = (expert * SLOTS + (lane // peers) % SLOTS).astype(F32)
    expert_sum = jnp.zeros((count, half), F32)
    for k in range(SLOTS):
        pick = jnp.where(info[:, k : k + 1] == code, 1.0, 0.0).astype(BF16)
        expert_sum += column(weight[k : k + 1, :], count) * mm(pick, values)
    square = jnp.sum(returned[:, rows : rows + 8, :].astype(F32), axis=0)
    square = column(square[0:1, :count], count)
    dense = jnp.sum(parts[...].astype(F32), axis=0)
    dense = (dense * lax.rsqrt(square / FF2 + EPS)).astype(BF16).astype(F32)
    out[...] = (resid[...].astype(F32) + expert_sum + branch[:, :1] * dense).astype(BF16)


def last_sum(returned, parts, info, weight, branch, resid):
    arrays = (returned, parts, info, weight, branch, resid)
    out = jax.ShapeDtypeStruct(resid.shape, BF16)
    scratch = [pltpu.VMEM((returned.shape[0], 2 * SLOTS * resid.shape[1] // LANES, LANES), F32)]
    return near_call(last_kernel, arrays, out, scratch, limit=16)


def body(
    tokens,
    norm_gain,
    query_w,
    key_w,
    value_w,
    forget_w,
    forget_bias,
    query_gain,
    key_gain,
    cache_key,
    cache_value,
    cache_gate,
    cache_len,
    out_w,
    post_gain,
    branch_gate,
    dense_gate_w,
    dense_up_w,
    dense_down_w,
    expert_choice,
    route_weight,
    expert_gate_w,
    expert_up_w,
    expert_down_w,
):
    count = tokens.shape[0]
    ep_count = lax.axis_size("ep")
    peers = ep_count // 2
    pair = [(e, e ^ 1) for e in range(ep_count)]
    classes = [[e for e in range(ep_count) if class_of(e) == c] for c in range(2)]

    near = []
    for array in (dense_gate_w, dense_up_w, dense_down_w):
        near.append(lax.ppermute(array, "ep", pair))

    partial, fresh_key, fresh_value, current = attend(
        cache_len, tokens, tiled(norm_gain), query_w, key_w, value_w, forget_w.T,
        forget_bias[None], query_gain[None], key_gain[None], cache_key, cache_value,
        cache_gate, out_w,
    )
    partial_other = swapped(partial)
    info = route(expert_choice.T)
    copies, resid, branch = normalize(
        tokens, partial, partial_other, tiled(post_gain), tiled(branch_gate), info, peers
    )
    lines = lax.all_to_all(copies, "ep", 0, 0, tiled=True, axis_index_groups=classes)
    lines = lines.reshape(peers * count, -1)

    gate_up = []
    for array in (dense_gate_w, dense_up_w, near[0], near[1]):
        gate_up += [array, swapped(array)]
    downs = []
    for down_w in (dense_down_w, near[2]):
        downs += [down_w, swapped(down_w)]

    width, units = dense_gate_w.shape
    far_wide = pack(pack_kernel, gate_up[4:], (width // 2, 4 * units))
    own_wide = pack(pack_kernel, gate_up[:4], (width // 2, 4 * units))
    down = pack(pack_down_kernel, downs, (len(downs) * units, width // 2))
    part = dense_hidden(lines, own_wide, far_wide)
    part_other = swapped(part)
    own_rows, near_rows = extract(lines, count)
    pair_rows = lax.ppermute(near_rows, "ep", pair)
    terms, squares = dense_down(part, part_other, down, count)
    parts = lax.all_to_all(
        terms.reshape(peers, count, -1), "ep", 0, 0, tiled=True, axis_index_groups=classes
    )

    away = (swapped(own_rows), swapped(pair_rows))
    keep, give = experts(
        (own_rows, pair_rows), away, expert_gate_w, expert_up_w, expert_down_w, squares
    )
    other = swapped(give)
    back = lax.ppermute(merge(keep, other), "ep", pair)
    answer = answers(keep, other, back, squares)
    returned = lax.all_to_all(answer, "ep", 0, 0, tiled=True, axis_index_groups=classes)
    mixed_out = last_sum(returned, parts, info, route_weight.T, branch, resid)
    return (mixed_out, fresh_key[:, None, :], fresh_value[:, None, :], current)


def solution(mesh):
    placed = (
        P("ep", None),
        P(),
        P(None, "tp"),
        P(),
        P(),
        P(),
        P(),
        P(),
        P(),
        P("ep", "tp", None, None),
        P("ep", "tp", None, None),
        P("ep", "tp", None),
        P("ep"),
        P("tp", None),
        P(),
        P(),
        P(None, ("ep", "tp")),
        P(None, ("ep", "tp")),
        P(("ep", "tp"), None),
        P("ep", None),
        P("ep", None),
        P("ep", None, "tp"),
        P("ep", None, "tp"),
        P("ep", "tp", None),
    )

    return jax.shard_map(
        body,
        mesh=mesh,
        in_specs=placed,
        out_specs=(P("ep", "tp"), P("ep", "tp", None), P("ep", "tp", None), P("ep", "tp")),
        check_vma=False,
    )
```
